512 devices in a mesh: row: 64 (over z, y), col: 8 (over x, core).
Axes of the slice: x: 4, y: 8, z: 8, core: 2. Of those that a mesh axis runs over, the one named last changes fastest.
Arguments:
- tokens: bfloat16 [8, 24576, 2048], P('col', 'row'), may hold values from -6 to 6
- norm_gain: bfloat16 [2048], replicated, may hold values from 0.099609375 to 1.8984375
- in_weight: bfloat16 [2048, 512], P('row', 'col'), may hold values from -0.125 to 0.125
- out_weight: bfloat16 [512, 2048], P('col', 'row'), may hold values from -0.25 to 0.25
Outputs:
- mixed: bfloat16 [8, 24576, 2048], P('col', 'row')
The draws below stay inside these ranges and needn't reach their ends.
All inputs are finite; a program needn't handle non-finite values.
Results may differ from the reference program's by a relative error of at most 0.013.
Values may be sent and summed in bfloat16 or wider, within the bound.
A program may use at most 64 MiB of HBM per device.

```python
import jax
import jax.numpy as jnp
from jax import lax

D = 2048
FW = 512
GS = 64
GROUPS = 8
LEN = 24576
BATCH = 8


def block_scale(stream_key, extent, pieces, smallest, largest):
    def one(dim, parts):
        steps = jax.random.uniform(jax.random.fold_in(jax.random.fold_in(stream_key, 6), dim), (parts,), jnp.float32, smallest / len(pieces), largest / len(pieces))
        return jnp.repeat(jnp.exp(steps), extent[dim] // parts).reshape((-1,) + (1,) * (len(extent) - dim - 1))

    level = one(*pieces[0])
    for cut in pieces[1:]:
        level = level * one(*cut)
    return level


def bell_draw(key, extent, spread, limit, cuts=(), dtype=jnp.bfloat16):
    loudness = block_scale(key, extent, cuts, -0.22, 0.18) if cuts else 1.0
    values = jax.random.normal(key, extent, jnp.float32) * spread * loudness
    return jnp.minimum(jnp.maximum(values, -limit), limit).astype(dtype)


def setup_inputs(seed: int = 0) -> dict:
    streams_of = jax.random.split(jax.random.key(seed), 5)
    tokens = bell_draw(streams_of[0], (BATCH, LEN, D), 1.0, 6.0, ((0, 8), (1, 64)))
    norm_gain = jnp.clip(1.0 + 0.18 * jax.random.normal(streams_of[1], (D,), jnp.float32), 0.099609375, 1.8984375).astype(jnp.bfloat16)
    in_weight = bell_draw(streams_of[2], (D, FW), D ** -0.5, 0.125, ((0, 64), (1, 8)))
    out_weight = bell_draw(streams_of[3], (FW, D), FW ** -0.5, 0.25, ((0, 8), (1, 64)))
    return {"tokens": tokens, "norm_gain": norm_gain, "in_weight": in_weight, "out_weight": out_weight}


EPS = 1e-06

def mix_sequence(sequence, norm_gain, in_weight, out_weight):
    widened = sequence.astype(jnp.float32)
    inverse_rms = lax.rsqrt(lax.optimization_barrier(jnp.mean(widened * widened, axis=-1, keepdims=True)) + EPS)
    normed = (widened * inverse_rms * norm_gain.astype(jnp.float32)).astype(jnp.bfloat16)
    projected = jnp.dot(normed, in_weight, preferred_element_type=jnp.float32).astype(jnp.bfloat16)
    grouped = projected.astype(jnp.float32).reshape(LEN, GROUPS, GS)
    spectrum = jnp.fft.fftn(grouped, axes=(0, 2), norm='ortho')
    mixed_real = jnp.real(spectrum).reshape(LEN, FW).astype(jnp.bfloat16)
    return jnp.dot(mixed_real, out_weight, preferred_element_type=jnp.float32).astype(jnp.bfloat16)

def reference(tokens, norm_gain, in_weight, out_weight):
    return lax.map(lambda sequence: mix_sequence(sequence, norm_gain, in_weight, out_weight), tokens)
```

```python
import functools
import math

import jax
import jax.numpy as jnp
import numpy as np
from jax import lax
from jax.experimental import pallas as pl
from jax.experimental.pallas import tpu as pltpu
from jax.sharding import PartitionSpec as P

GS = 64
HALF = GS // 2
EPS = 1e-06
F32 = jnp.float32
BF16 = jnp.bfloat16
MESH = pl.DeviceIdType.MESH


class Sizes:
    def __init__(self, rows, cols, local, width):
        self.rows = rows
        self.nz = 1 << ((rows.bit_length() - 1 + 1) // 2)
        self.ny = rows // self.nz
        self.nx = cols // 2
        self.local = local
        self.width = width
        self.ch = GS * self.nx
        self.per = 2 * self.ch // rows
        self.pairs = self.per // 2
        self.hops = local // rows
        self.blk = width // rows
        self.tiles = max(1, local // 128)
        self.lane = local // self.tiles


def tables(z):
    rows, local, ch = z.rows, z.local, z.ch
    length = rows * local
    k = np.arange(GS)
    small = np.zeros((GS, GS))
    for j in range(HALF):
        if j == 0:
            small[0] = (1.0 + (-1.0) ** k) / 2
            small[1] = (1.0 - (-1.0) ** k) / 2
        else:
            small[2 * j] = np.cos(2 * math.pi * j * k / GS)
            small[2 * j + 1] = np.sin(2 * math.pi * j * k / GS)
    chan = np.kron(np.eye(z.nx), small)
    i = np.arange(rows)
    ang = 2 * math.pi * np.outer(i, i) / rows
    c, s = np.cos(ang), np.sin(ang)
    first = np.stack(
        [
            np.block([[c, -s], [-s, -c], [c, s], [-s, c]]),
            np.block([[c, c], [-s, -s], [c, -c], [-s, s]]),
        ]
    )
    m = np.arange(local)
    tw = 2 * math.pi * np.outer(i, m) / length
    turn = np.stack([np.cos(tw), np.sin(tw)])
    a = np.arange(z.hops)
    k2 = (z.hops * i[None, :] + a[:, None]).reshape(-1)
    ang2 = 2 * math.pi * (np.outer(k2, m) % local) / local
    scale = 1.0 / math.sqrt(length * GS)
    second = np.concatenate([np.cos(ang2), np.sin(ang2)], axis=1) * scale
    place_in = np.zeros((z.nx, 2 * GS, ch))
    place_out = np.zeros((z.nx, 2 * GS, ch))
    for x in range(z.nx):
        for q in range(GS):
            place_in[x, q, GS * x + q] = 1
        for j in range(HALF):
            place_out[x, GS + j, GS * x + 2 * j] = 1
            other = HALF if j == 0 else GS - j
            place_out[x, GS + other, GS * x + 2 * j + 1] = 1
    bf = lambda t: jnp.asarray(t.astype(np.float32)).astype(BF16)
    return (
        bf(chan),
        bf(first),
        jnp.asarray(turn.astype(np.float32)),
        bf(second),
        bf(place_in),
        bf(place_out),
    )


def dot(a, b):
    return jnp.dot(a, b, preferred_element_type=F32)


def dot_nt(a, b):
    return lax.dot_general(a, b, (((1,), (1,)), ((), ())), preferred_element_type=F32)


def kernel(
    z,
    tok_hbm, gain_ref, blk_ref, chan_hbm, first_hbm, turn_hbm, second_hbm, pin_hbm, pout_hbm,
    out_hbm,
    tok, chan, first, turn, second, pin, pout,
    xbuf, win, wo, ht, got, stage, gp, back, got2, obuf,
    tab_sem, tok_sem, swap_send, swap_recv,
    x_send, x_recv, in_send, in_recv, wo_send, wo_recv, half_send, half_recv,
    a_send, a_recv, b_send, b_recv, o_sem,
):
    rows, ny, nz, nx, local = z.rows, z.ny, z.nz, z.nx, z.local
    r = lax.axis_index("row")
    c = lax.axis_index("col")
    h = lax.rem(c, 2)
    x = c // 2
    zz = r // ny
    yy = lax.rem(r, ny)
    other = c + 1 - 2 * h

    def send(src, dst, ssem, rsem, row, col):
        copy = pltpu.make_async_remote_copy(
            src_ref=src, dst_ref=dst, send_sem=ssem, recv_sem=rsem,
            device_id=(row, col), device_id_type=MESH,
        )
        copy.start()

    def drain(ref, sem):
        pltpu.make_async_copy(ref, ref, sem).wait()

    barrier = pltpu.get_barrier_semaphore()

    def greet(i, carry):
        peer = lax.rem(r + i, rows)
        pl.semaphore_signal(barrier, inc=1, device_id=(peer, c), device_id_type=MESH)
        pl.semaphore_signal(barrier, inc=1, device_id=(peer, other), device_id_type=MESH)
        return carry

    for d in range(1, nx):
        px = lax.rem(x + d, nx)
        pl.semaphore_signal(barrier, inc=1, device_id=(r, 2 * px + h), device_id_type=MESH)
    pl.semaphore_signal(barrier, inc=1, device_id=(r, other), device_id_type=MESH)
    lax.fori_loop(1, rows, greet, 0)

    own = pltpu.make_async_copy(tok_hbm, tok.at[h], tok_sem)
    own.start()
    loads = [
        pltpu.make_async_copy(src, dst, tab_sem.at[n])
        for n, (src, dst) in enumerate(
            [(pin_hbm, pin), (pout_hbm, pout), (chan_hbm, chan), (first_hbm, first),
             (turn_hbm, turn), (second_hbm, second)]
        )
    ]
    for load in loads:
        load.start()
    pl.semaphore_wait(barrier, 2 * rows - 1 + nx - 1)

    for d in range(1, nx):
        px = lax.rem(x + d, nx)
        send(blk_ref, xbuf.at[x], x_send, x_recv, r, 2 * px + h)
    send(tok_hbm, tok.at[h], swap_send, swap_recv, r, other)
    xbuf[x] = blk_ref[...]
    loads[0].wait()
    loads[1].wait()
    drain(xbuf.at[pl.ds(0, nx - 1)], x_recv)

    def assemble(place):
        total = dot(xbuf[0], place[0])
        for n in range(1, nx):
            total += dot(xbuf[n], place[n])
        return total.astype(BF16)

    win[zz, yy] = assemble(pin)
    wo[h, zz, yy] = assemble(pout)

    hb = z.blk // 2
    lo, hi = pl.ds(0, hb), pl.ds(hb, hb)
    wh = wo.at[h]
    for buf, ssem, rsem in ((win, in_send, in_recv), (wh, wo_send, wo_recv)):
        for d in range(1, ny):
            py = lax.rem(yy + d, ny)
            send(buf.at[zz, yy, lo], buf.at[zz, yy, lo], ssem.at[0], rsem.at[0], zz * ny + py, c)
        for d in range(1, nz):
            pz = lax.rem(zz + d, nz)
            send(buf.at[zz, yy, hi], buf.at[zz, yy, hi], ssem.at[1], rsem.at[1], pz * ny + yy, c)

    gain = gain_ref[...].astype(F32)
    step = min(32, local)

    def norm(q):
        def one(i, carry):
            part = pl.ds(pl.multiple_of(i * step, step), step)
            v = tok[q, part, :].astype(F32)
            inv = lax.rsqrt(jnp.mean(v * v, axis=-1, keepdims=True) + EPS)
            tok[q, part, :] = (v * inv * gain).astype(BF16)
            return carry

        lax.fori_loop(0, local // step, one, 0)

    for buf, ssem, rsem in ((win, in_send, in_recv), (wh, wo_send, wo_recv)):
        drain(buf.at[0, pl.ds(0, ny - 1), lo], rsem.at[0])
        drain(buf.at[pl.ds(0, nz - 1), 0, hi], rsem.at[1])
        for d in range(1, nz):
            pz = lax.rem(zz + d, nz)
            send(buf.at[zz, :, lo], buf.at[zz, :, lo], ssem.at[2], rsem.at[2], pz * ny + yy, c)
        for d in range(1, ny):
            py = lax.rem(yy + d, ny)
            send(buf.at[:, yy, hi], buf.at[:, yy, hi], ssem.at[3], rsem.at[3], zz * ny + py, c)

    own.wait()
    norm(h)
    drain(tok.at[0], swap_recv)
    norm(1 - h)
    drain(win.at[pl.ds(0, nz - 1), :, lo], in_recv.at[2])
    drain(win.at[:, pl.ds(0, ny - 1), hi], in_recv.at[3])
    loads[2].wait()

    groups = rows // 2
    weight = win[...].reshape(z.width, z.ch)
    for q in range(2):
        proj = dot(tok[q], weight).astype(BF16)
        cols = dot_nt(chan[...], proj).astype(BF16)
        ht[pl.ds(groups * q, groups)] = cols.reshape(groups, z.per, local)

    def scatter(i, carry):
        peer = lax.rem(r + i, rows)
        send(ht.at[peer], got.at[r], a_send, a_recv, peer, c)
        return carry

    lax.fori_loop(1, rows, scatter, 0)
    got[r] = ht[r]
    for load in loads[3:]:
        load.wait()

    drain(wh.at[pl.ds(0, nz - 1), :, lo], wo_recv.at[2])
    drain(wh.at[:, pl.ds(0, ny - 1), hi], wo_recv.at[3])
    send(wh, wh, half_send, half_recv, r, other)

    drain(got.at[pl.ds(0, rows - 1)], a_recv)

    lane = z.lane
    for l in range(z.tiles):
        part = got[:, :, l * lane:(l + 1) * lane].astype(F32)
        stage[l] = part.reshape(rows * z.per, lane)
    odd = lax.rem(lax.rem(r, groups) * z.pairs, HALF)
    tc, ts = turn[0], turn[1]
    for p in range(z.pairs):
        if p == 0:
            matrix = jnp.where(odd == 0, first[1].astype(F32), first[0].astype(F32)).astype(BF16)
        else:
            matrix = first[0]
        for l in range(z.tiles):
            lanes = slice(l * lane, (l + 1) * lane)
            cos, sin = tc[:, lanes], ts[:, lanes]
            u = stage[l, pl.ds(2 * p, rows, stride=z.per), :]
            v = stage[l, pl.ds(2 * p + 1, rows, stride=z.per), :]
            g = dot(matrix, jnp.concatenate([u, v], axis=0).astype(BF16))
            for w in range(2):
                re = g[2 * w * rows:(2 * w + 1) * rows]
                im = g[(2 * w + 1) * rows:(2 * w + 2) * rows]
                at = pl.ds((2 * p + w) * rows, rows)
                gp[at, l * lane:(l + 1) * lane] = (re * cos + im * sin).astype(BF16)
                gp[at, local + l * lane:local + (l + 1) * lane] = (im * cos - re * sin).astype(BF16)
    spec = dot_nt(second[...], gp[...])
    if rows == GS and lane == 128:
        left = lax.broadcasted_iota(jnp.int32, (rows, lane), 1) < rows
        for l in range(z.tiles):
            for p in range(z.pairs):
                t0 = spec[2 * l * rows:(2 * l + 1) * rows, p * lane:(p + 1) * lane]
                t1 = spec[(2 * l + 1) * rows:(2 * l + 2) * rows, p * lane:(p + 1) * lane]
                stage[l, pl.ds(2 * p, rows, stride=z.per), :] = jnp.where(
                    left, t0, pltpu.roll(t1, rows, 1)
                )
                stage[l, pl.ds(2 * p + 1, rows, stride=z.per), :] = jnp.where(
                    left, pltpu.roll(t0, rows, 1), t1
                )
    else:
        full = spec.reshape(z.hops, rows, z.per, rows).transpose(1, 2, 0, 3)
        full = full.reshape(rows * z.per, z.tiles, lane)
        for l in range(z.tiles):
            stage[l] = full[:, l]
    for l in range(z.tiles):
        back[:, :, l * lane:(l + 1) * lane] = stage[l].reshape(rows, z.per, lane).astype(BF16)

    seq = r // groups
    slot = h * groups + lax.rem(r, groups)
    target = 2 * x + seq

    def give(i, carry):
        peer = lax.rem(r + i, rows)
        send(back.at[peer], got2.at[slot], b_send, b_recv, peer, target)
        return carry

    lax.fori_loop(1, rows, give, 0)

    @pl.when(seq == h)
    def _():
        got2[slot] = back[r]

    @pl.when(seq != h)
    def _():
        send(back.at[r], got2.at[slot], b_send, b_recv, r, target)

    drain(wo.at[0], half_recv)

    @pl.when(seq == h)
    def _():
        drain(got2.at[pl.ds(0, rows - 1)], b_recv)

    @pl.when(seq != h)
    def _():
        drain(got2, b_recv)

    mixed = got2[...].astype(F32).reshape(rows * z.per, local).T.astype(BF16)
    ma, mb = mixed[:, :z.ch], mixed[:, z.ch:]
    chunk = ny * z.blk
    for n in range(nz):
        res = dot_nt(ma, wo[0, n].reshape(chunk, z.ch)) + dot_nt(mb, wo[1, n].reshape(chunk, z.ch))
        obuf[n] = res.astype(BF16)
        pltpu.make_async_copy(obuf.at[n], out_hbm.at[:, pl.ds(n * chunk, chunk)], o_sem.at[n]).start()
    for n in range(nz):
        pltpu.make_async_copy(obuf.at[n], out_hbm.at[:, pl.ds(n * chunk, chunk)], o_sem.at[n]).wait()

    drain(xbuf.at[pl.ds(0, nx - 1)], x_send)
    drain(tok.at[0], swap_send)
    for buf, ssem in ((win, in_send), (wh, wo_send)):
        drain(buf.at[0, pl.ds(0, ny - 1), lo], ssem.at[0])
        drain(buf.at[pl.ds(0, nz - 1), 0, hi], ssem.at[1])
        drain(buf.at[pl.ds(0, nz - 1), :, lo], ssem.at[2])
        drain(buf.at[:, pl.ds(0, ny - 1), hi], ssem.at[3])
    drain(wo.at[0], half_send)
    drain(ht.at[pl.ds(0, rows - 1)], a_send)

    @pl.when(seq == h)
    def _():
        drain(back.at[pl.ds(0, rows - 1)], b_send)

    @pl.when(seq != h)
    def _():
        drain(back, b_send)


def body(rows, cols, tokens, norm_gain, in_weight, out_weight):
    local, width = tokens.shape[1:]
    z = Sizes(rows, cols, local, width)
    block = jnp.concatenate([in_weight, out_weight.T], axis=1)
    consts = tables(z)
    any_spec = pl.BlockSpec(memory_space=pl.ANY)
    vmem = pl.BlockSpec(memory_space=pltpu.VMEM)
    scratch = [pltpu.VMEM((2, local, width), BF16)]
    scratch += [pltpu.VMEM(t.shape, t.dtype) for t in (consts[0], consts[1], consts[2], consts[3], consts[4], consts[5])]
    scratch += [
        pltpu.VMEM((z.nx, z.blk, 2 * GS), BF16),
        pltpu.VMEM((z.nz, z.ny, z.blk, z.ch), BF16),
        pltpu.VMEM((2, z.nz, z.ny, z.blk, z.ch), BF16),
        pltpu.VMEM((rows, z.per, local), BF16),
        pltpu.VMEM((rows, z.per, local), BF16),
        pltpu.VMEM((z.tiles, rows * z.per, z.lane), F32),
        pltpu.VMEM((z.per * rows, 2 * local), BF16),
        pltpu.VMEM((rows, z.per, local), BF16),
        pltpu.VMEM((rows, z.per, local), BF16),
        pltpu.VMEM((z.nz, local, z.ny * z.blk), BF16),
    ]
    dma = pltpu.SemaphoreType.DMA
    scratch += [dma((6,)), dma, dma, dma, dma, dma, dma((4,)), dma((4,)), dma((4,)), dma((4,)),
                dma, dma, dma, dma, dma, dma, dma((z.nz,))]
    mixed = pl.pallas_call(
        functools.partial(kernel, z),
        out_shape=jax.ShapeDtypeStruct((local, width), BF16),
        in_specs=[any_spec, vmem, vmem] + [any_spec] * 6,
        out_specs=any_spec,
        scratch_shapes=scratch,
        compiler_params=pltpu.CompilerParams(
            collective_id=0, has_side_effects=True, vmem_limit_bytes=60 * 1024 * 1024
        ),
        name="fourier_mix",
    )(tokens[0], norm_gain[None], block, *consts)
    return mixed[None]


def solution(mesh):
    rows, cols = mesh.shape["row"], mesh.shape["col"]
    in_specs = (P("col", "row", None), P(), P("row", "col"), P("col", "row"))
    return jax.shard_map(
        functools.partial(body, rows, cols), mesh=mesh, in_specs=in_specs,
        out_specs=P("col", "row", None), check_vma=False,
    )
```

```python
import functools
import math

import jax
import jax.numpy as jnp
import numpy as np
from jax import lax
from jax.experimental import pallas as pl
from jax.experimental.pallas import tpu as pltpu
from jax.sharding import PartitionSpec as P

GS = 64
HALF = GS // 2
EPS = 1e-06
F32 = jnp.float32
BF16 = jnp.bfloat16
MESH = pl.DeviceIdType.MESH
VMEM_LIMIT = 52 * 1024 * 1024


class Sizes:
    def __init__(self, rows, cols, local, width):
        self.rows = rows
        self.nz = 1 << ((rows.bit_length() - 1 + 1) // 2)
        self.ny = rows // self.nz
        self.nx = cols // 2
        self.local = local
        self.width = width
        self.ch = GS * self.nx
        self.per = 2 * self.ch // rows
        self.pairs = self.per // 2
        self.hops = local // rows
        self.blk = width // rows
        self.cut = 4
        self.tiles = max(1, local // 128)
        self.lane = local // self.tiles


def tables(z):
    rows, local, ch = z.rows, z.local, z.ch
    length = rows * local
    k = np.arange(GS)
    small = np.zeros((GS, GS))
    for j in range(HALF):
        if j == 0:
            small[0] = (1.0 + (-1.0) ** k) / 2
            small[1] = (1.0 - (-1.0) ** k) / 2
        else:
            small[2 * j] = np.cos(2 * math.pi * j * k / GS)
            small[2 * j + 1] = np.sin(2 * math.pi * j * k / GS)
    chan = np.kron(np.eye(z.nx), small)
    i = np.arange(rows)
    ang = 2 * math.pi * (np.outer(i, i) % rows) / rows
    c, s = np.cos(ang), np.sin(ang)
    first = np.concatenate(
        [
            np.block([[c, -s], [-s, -c], [c, s], [-s, c]]),
            np.block([[c, c], [-s, -s], [c, -c], [-s, s]]),
        ]
    )
    m = np.arange(local)
    tw = 2 * math.pi * np.outer(i, m) / length
    turn = np.concatenate([np.cos(tw), np.sin(tw)]).astype(np.float32)
    high = turn.astype(BF16).astype(np.float32)
    turn = np.concatenate([high, turn - high], axis=1)
    a = np.arange(z.hops)
    k2 = (z.hops * i[None, :] + a[:, None]).reshape(-1)
    ang2 = 2 * math.pi * (np.outer(k2, m) % local) / local
    second = np.concatenate([np.cos(ang2), np.sin(ang2)], axis=1) / math.sqrt(length * GS)
    parts = []
    for part in (second, first, chan, turn):
        wide = np.zeros((part.shape[0], 2 * local), np.float32)
        wide[:, : part.shape[1]] = part
        parts.append(wide)
    return jnp.asarray(np.concatenate(parts).astype(BF16))


def dot(a, b):
    return jnp.dot(a, b, preferred_element_type=F32)


def dot_nt(a, b):
    return lax.dot_general(a, b, (((1,), (1,)), ((), ())), preferred_element_type=F32)


def placed(rows, cols, target, keep):
    to = lax.broadcasted_iota(jnp.int32, (rows, cols), 1)
    return jnp.where((to == target) & keep, 1.0, 0.0).astype(BF16)


def kernel(
    z,
    tok_hbm, gain_hbm, wi_hbm, wt_hbm, tab_hbm,
    out,
    gain_ref, wi_ref, wt_ref, tab, tok,
    xbuf, win, wpk, wo, spread, ht, got, stage, gp, back, got2,
    tab_sem, tok_sem, swap_send, swap_recv,
    x_send, x_recv, in_send, in_recv, ring_recv, wo_send, wo_recv,
    far_send, far_recv, half_send, half_recv,
    a_send, a_recv, b_send, b_recv,
):
    rows, ny, nz, nx, local = z.rows, z.ny, z.nz, z.nx, z.local
    groups = rows // 2
    r = lax.axis_index("row")
    c = lax.axis_index("col")
    h = lax.rem(c, 2)
    x = c // 2
    zz = r // ny
    yy = lax.rem(r, ny)
    other = c + 1 - 2 * h

    def send(src, dst, ssem, rsem, row, col):
        copy = pltpu.make_async_remote_copy(
            src_ref=src, dst_ref=dst, send_sem=ssem, recv_sem=rsem,
            device_id=(row, col), device_id_type=MESH,
        )
        copy.start()

    def drain(ref, sem):
        pltpu.make_async_copy(ref, ref, sem).wait()

    barrier = pltpu.get_barrier_semaphore()
    loads = [
        pltpu.make_async_copy(src, dst, tab_sem.at[n])
        for n, (src, dst) in enumerate(
            [(wi_hbm, wi_ref), (wt_hbm, wt_ref), (gain_hbm, gain_ref), (tab_hbm, tab)]
        )
    ]
    for load in loads[:2]:
        load.start()

    def greet(i, carry):
        peer = lax.rem(r + i, rows)
        pl.semaphore_signal(barrier, inc=1, device_id=(peer, c), device_id_type=MESH)
        pl.semaphore_signal(barrier, inc=1, device_id=(peer, other), device_id_type=MESH)
        return carry

    for d in range(1, nx):
        px = lax.rem(x + d, nx)
        pl.semaphore_signal(barrier, inc=1, device_id=(r, 2 * px + h), device_id_type=MESH)
    pl.semaphore_signal(barrier, inc=1, device_id=(r, other), device_id_type=MESH)
    lax.fori_loop(1, rows, greet, 0)

    own = pltpu.make_async_copy(tok_hbm, tok.at[h], tok_sem)
    own.start()
    for load in loads[2:]:
        load.start()
    packed = 2 * GS
    at = lax.broadcasted_iota(jnp.int32, (nx * packed, z.ch), 0)
    for half in range(2):
        q = lax.rem(at, packed) - GS * half
        place = jnp.where(q < HALF, 2 * q, 2 * GS + 1 - 2 * q)
        place = jnp.where(q == HALF, 1, place) + GS * (at // packed)
        spread[half] = placed(nx * packed, z.ch, place, (q >= 0) & (q < GS))
    loads[0].wait()
    loads[1].wait()
    hb = z.blk // 2
    lo, hi = pl.ds(0, hb), pl.ds(hb, hb)
    side = lax.broadcasted_iota(jnp.int32, (GS, packed), 0)
    everywhere = side >= 0
    wpk[h, x, zz, yy] = (
        dot(wt_ref[:hb], placed(GS, packed, side, everywhere))
        + dot(wt_ref[hb:], placed(GS, packed, side + GS, everywhere))
    ).astype(BF16)
    xbuf[x] = wi_ref[...]
    pl.semaphore_wait(barrier, 2 * rows - 1 + nx - 1)

    for d in range(1, nx):
        px = lax.rem(x + d, nx)
        send(wi_ref, xbuf.at[x], x_send, x_recv, r, 2 * px + h)
    send(tok_hbm, tok.at[h], swap_send, swap_recv, r, other)
    chan_at = lax.broadcasted_iota(jnp.int32, (GS, z.ch), 0)
    drain(xbuf.at[pl.ds(0, nx - 1)], x_recv)
    total = dot(xbuf[0], placed(GS, z.ch, chan_at, chan_at >= 0))
    for n in range(1, nx):
        total += dot(xbuf[n], placed(GS, z.ch, chan_at + GS * n, chan_at >= 0))
    win[zz, yy] = total.astype(BF16)

    for d in range(1, ny):
        py = lax.rem(yy + d, ny)
        send(win.at[zz, yy, lo], win.at[zz, yy, lo], in_send.at[0], in_recv.at[0], zz * ny + py, c)
    for d in range(1, nz):
        pz = lax.rem(zz + d, nz)
        send(win.at[zz, yy, hi], win.at[zz, yy, hi], in_send.at[1], in_recv.at[1], pz * ny + yy, c)
    mine = wpk.at[h, x]

    @pl.when(h == 0)
    def _():
        for d in range(1, ny):
            py = lax.rem(yy + d, ny)
            send(mine.at[zz, yy], mine.at[zz, yy], wo_send.at[0], wo_recv.at[0], zz * ny + py, c)

    @pl.when(h == 1)
    def _():
        for d in range(1, nz):
            pz = lax.rem(zz + d, nz)
            send(mine.at[zz, yy], mine.at[zz, yy], wo_send.at[0], wo_recv.at[0], pz * ny + yy, c)

    loads[2].wait()
    gain = gain_ref[...].astype(F32).reshape(1, z.width)
    step = min(32, local)

    def norm(q):
        def one(i, carry):
            part = pl.ds(pl.multiple_of(i * step, step), step)
            v = tok[q, part, :].astype(F32)
            inv = lax.rsqrt(jnp.mean(v * v, axis=-1, keepdims=True) + EPS)
            tok[q, part, :] = (v * inv * gain).astype(BF16)
            return carry

        lax.fori_loop(0, local // step, one, 0)

    own.wait()
    norm(h)

    drain(win.at[0, pl.ds(0, ny - 1), lo], in_recv.at[0])
    drain(win.at[pl.ds(0, nz - 1), 0, hi], in_recv.at[1])
    cy, cz = min(z.cut, ny), min(z.cut, nz)

    def low(block, chunk):
        return win.at[block, pl.ds(chunk * (ny // cy), ny // cy), lo]

    def high(block, chunk):
        return win.at[pl.ds(chunk * (nz // cz), nz // cz), block, hi]

    def row_z(p):
        return p * ny + yy

    def row_y(p):
        return zz * ny + p

    paths = ((low, nz, zz, cy, row_z), (high, ny, yy, cz, row_y))

    def carried(n, cut, hop, sign):
        if hop < n // 2:
            return range(cut)
        return range(cut // 2) if sign > 0 else range(cut // 2, cut)

    longest = max(nz, ny) // 2

    def advance(hop):
        for chunk in range(max(cy, cz)):
            for p, (view, n, pos, cut, row) in enumerate(paths):
                for e, sign in enumerate((1, -1)):
                    block = lax.rem(pos - sign * (hop - 1) + n, n)
                    if 1 < hop <= n // 2 + 1 and chunk in carried(n, cut, hop - 1, sign):
                        drain(view(block, chunk), ring_recv.at[p, e, hop - 2, chunk])
                    if hop <= n // 2 and chunk in carried(n, cut, hop, sign):
                        to = lax.rem(pos + sign + n, n)
                        send(view(block, chunk), view(block, chunk), in_send.at[2 + p],
                             ring_recv.at[p, e, hop - 1, chunk], row(to), c)

    advance(1)

    @pl.when(h == 0)
    def _():
        drain(wpk.at[0, 0, 0, pl.ds(0, ny - 1)], wo_recv.at[0])
        for d in range(1, nz):
            pz = lax.rem(zz + d, nz)
            send(mine.at[zz], mine.at[zz], wo_send.at[1], wo_recv.at[1], pz * ny + yy, c)

    @pl.when(h == 1)
    def _():
        drain(wpk.at[0, 0, pl.ds(0, nz - 1), 0], wo_recv.at[0])
        for d in range(1, ny):
            py = lax.rem(yy + d, ny)
            send(mine.at[:, yy], mine.at[:, yy], wo_send.at[1], wo_recv.at[1], zz * ny + py, c)

    drain(tok.at[0], swap_recv)
    norm(1 - h)
    for hop in range(2, longest + 2):
        with jax.named_scope(f"pring{hop}"):
            advance(hop)

    @pl.when(h == 0)
    def _():
        drain(wpk.at[0, 0, pl.ds(0, nz - 1)], wo_recv.at[1])

    @pl.when(h == 1)
    def _():
        drain(wpk.at[0, 0, :, pl.ds(0, ny - 1)], wo_recv.at[1])

    near = (1, nx - 1) if nx == 4 else tuple(range(1, nx))
    for n, d in enumerate(near):
        px = lax.rem(x + d, nx)
        send(mine, mine, far_send, far_recv.at[n], r, 2 * px + h)
    send(mine, mine, half_send, half_recv.at[0], r, other)

    loads[3].wait()
    o1 = local
    o2 = o1 + 8 * rows
    o3 = o2 + z.ch
    chan = tab[o2:o3, :z.ch]
    weight = win[...].reshape(z.width, z.ch)
    for q in range(2):
        proj = dot(tok[q], weight).astype(BF16)
        cols = dot_nt(chan, proj).astype(BF16)
        ht[pl.ds(groups * q, groups)] = cols.reshape(groups, z.per, local)

        def scatter(i, carry):
            peer = groups * q + lax.rem(r + i, groups)

            @pl.when(peer != r)
            def _():
                send(ht.at[peer], got.at[r], a_send, a_recv, peer, c)

            return carry

        lax.fori_loop(0, groups, scatter, 0)
    got[r] = ht[r]

    zh = nz // 2
    for n, d in enumerate(near):
        theirs = wpk.at[h, lax.rem(x - d + nx, nx)]
        drain(theirs, far_recv.at[n])
        if nx == 4:
            part = pl.ds(n * zh, zh)
            to = lax.rem(x + d, nx)
            send(theirs.at[part], theirs.at[part], far_send, far_recv.at[2 + n], r, 2 * to + h)
        send(theirs, theirs, half_send, half_recv.at[1 + n], r, other)

    drain(got.at[pl.ds(0, rows - 1)], a_recv)

    lane = z.lane
    for l in range(z.tiles):
        part = got[:, :, l * lane:(l + 1) * lane].astype(F32)
        stage[l] = part.reshape(rows * z.per, lane)
    base = lax.rem(r, groups) * z.pairs
    plain = tab[o1:o1 + 4 * rows, :2 * rows]
    for p in range(z.pairs):
        matrix = plain
        if p % min(z.pairs, HALF) == 0:
            paired = tab[o1 + 4 * rows:o2, :2 * rows].astype(F32)
            special = lax.rem(base + p, HALF) == 0
            matrix = jnp.where(special, paired, plain.astype(F32)).astype(BF16)
        for l in range(z.tiles):
            lanes = slice(l * lane, (l + 1) * lane)
            rest = slice(local + l * lane, local + (l + 1) * lane)
            cos = tab[o3:o3 + rows, lanes].astype(F32) + tab[o3:o3 + rows, rest].astype(F32)
            sin = (tab[o3 + rows:o3 + 2 * rows, lanes].astype(F32)
                   + tab[o3 + rows:o3 + 2 * rows, rest].astype(F32))
            u = stage[l, pl.ds(2 * p, rows, stride=z.per), :]
            v = stage[l, pl.ds(2 * p + 1, rows, stride=z.per), :]
            g = dot(matrix, jnp.concatenate([u, v], axis=0).astype(BF16))
            for w in range(2):
                re = g[2 * w * rows:(2 * w + 1) * rows]
                im = g[(2 * w + 1) * rows:(2 * w + 2) * rows]
                at = pl.ds((2 * p + w) * rows, rows)
                gp[at, lanes] = (re * cos + im * sin).astype(BF16)
                gp[at, rest] = (im * cos - re * sin).astype(BF16)
    spec = dot_nt(tab[:local], gp[...])
    if rows == GS and lane == 128:
        left = lax.broadcasted_iota(jnp.int32, (rows, lane), 1) < rows
        for l in range(z.tiles):
            for p in range(z.pairs):
                t0 = spec[2 * l * rows:(2 * l + 1) * rows, p * lane:(p + 1) * lane]
                t1 = spec[(2 * l + 1) * rows:(2 * l + 2) * rows, p * lane:(p + 1) * lane]
                stage[l, pl.ds(2 * p, rows, stride=z.per), :] = jnp.where(
                    left, t0, pltpu.roll(t1, rows, 1)
                )
                stage[l, pl.ds(2 * p + 1, rows, stride=z.per), :] = jnp.where(
                    left, pltpu.roll(t0, rows, 1), t1
                )
    else:
        full = spec.reshape(z.hops, rows, z.per, rows).transpose(1, 2, 0, 3)
        full = full.reshape(rows * z.per, z.tiles, lane)
        for l in range(z.tiles):
            stage[l] = full[:, l]
    for l in range(z.tiles):
        back[:, :, l * lane:(l + 1) * lane] = stage[l].reshape(rows, z.per, lane).astype(BF16)

    seq = r // groups
    slot = h * groups + lax.rem(r, groups)
    target = 2 * x + seq

    def give(i, carry):
        peer = lax.rem(r + i, rows)
        send(back.at[peer], got2.at[slot], b_send, b_recv, peer, target)
        return carry

    lax.fori_loop(1, rows, give, 0)

    @pl.when(seq == h)
    def _():
        got2[slot] = back[r]

    @pl.when(seq != h)
    def _():
        send(back.at[r], got2.at[slot], b_send, b_recv, r, target)

    if nx == 4:
        far = lax.rem(x + 2, nx)
        for n in range(2):
            part = wpk.at[h, far, pl.ds(n * zh, zh)]
            drain(part, far_recv.at[2 + n])
            send(part, part, half_send, half_recv.at[3], r, other)

    def unpack(half_of):
        flat = jnp.concatenate(
            [wpk[half_of, n].reshape(rows * hb, packed) for n in range(nx)], axis=1
        )
        for half in range(2):
            sorted_ = dot(flat, spread[half]).astype(BF16)
            wo[half_of, :, half * hb:(half + 1) * hb, :] = sorted_.reshape(rows, hb, z.ch)

    unpack(h)
    for n in range(nx):
        drain(wpk.at[0, 0], half_recv.at[n])
    unpack(1 - h)

    @pl.when(seq == h)
    def _():
        drain(got2.at[pl.ds(0, rows - 1)], b_recv)

    @pl.when(seq != h)
    def _():
        drain(got2, b_recv)

    mixed = got2[...].astype(F32).reshape(rows * z.per, local).T.astype(BF16)
    ma, mb = mixed[:, :z.ch], mixed[:, z.ch:]
    chunk = ny * z.blk
    for n in range(nz):
        some = pl.ds(n * ny, ny)
        res = dot_nt(ma, wo[0, some].reshape(chunk, z.ch)) + dot_nt(mb, wo[1, some].reshape(chunk, z.ch))
        out[:, n * chunk:(n + 1) * chunk] = res.astype(BF16)

    drain(xbuf.at[pl.ds(0, nx - 1)], x_send)
    drain(tok.at[0], swap_send)
    drain(win.at[0, pl.ds(0, ny - 1), lo], in_send.at[0])
    drain(win.at[pl.ds(0, nz - 1), 0, hi], in_send.at[1])
    drain(win.at[pl.ds(0, nz - 1), :, lo], in_send.at[2])
    drain(win.at[:, pl.ds(0, ny - 1), hi], in_send.at[3])

    @pl.when(h == 0)
    def _():
        drain(wpk.at[0, 0, 0, pl.ds(0, ny - 1)], wo_send.at[0])
        drain(wpk.at[0, 0, pl.ds(0, nz - 1)], wo_send.at[1])

    @pl.when(h == 1)
    def _():
        drain(wpk.at[0, 0, pl.ds(0, nz - 1), 0], wo_send.at[0])
        drain(wpk.at[0, 0, :, pl.ds(0, ny - 1)], wo_send.at[1])

    drain(wpk.at[0, pl.ds(0, nx - 1)], far_send)
    drain(wpk.at[0], half_send)
    drain(ht.at[pl.ds(0, rows - 1)], a_send)

    @pl.when(seq == h)
    def _():
        drain(back.at[pl.ds(0, rows - 1)], b_send)

    @pl.when(seq != h)
    def _():
        drain(back, b_send)


def body(rows, cols, tokens, norm_gain, in_weight, out_weight):
    local, width = tokens.shape[1:]
    z = Sizes(rows, cols, local, width)
    table = tables(z)
    hbm = pl.BlockSpec(memory_space=pltpu.HBM)
    vmem = pl.BlockSpec(memory_space=pltpu.VMEM)
    hb = z.blk // 2
    dma = pltpu.SemaphoreType.DMA
    vm = pltpu.VMEM
    exchange = (rows, z.per, local)
    scratch = [
        vm((width,), BF16),
        vm((z.blk, GS), BF16),
        vm((z.blk, GS), BF16),
        vm(table.shape, BF16),
        vm((2, local, width), BF16),
        vm((z.nx, z.blk, GS), BF16),
        vm((z.nz, z.ny, z.blk, z.ch), BF16),
        vm((2, z.nx, z.nz, z.ny, hb, 2 * GS), BF16),
        vm((2, rows, z.blk, z.ch), BF16),
        vm((2, 2 * GS * z.nx, z.ch), BF16),
        vm(exchange, BF16),
        vm(exchange, BF16),
        vm((z.tiles, rows * z.per, z.lane), F32),
        vm((z.per * rows, 2 * local), BF16),
        vm(exchange, BF16),
        vm(exchange, BF16),
        dma((4,)), dma, dma, dma,
        dma, dma, dma((4,)), dma((2,)), dma((2, 2, max(z.ny, z.nz) // 2, z.cut)), dma((2,)), dma((2,)),
        dma, dma((4,)), dma, dma((4,)),
        dma, dma, dma, dma,
    ]
    operands = (tokens[0], norm_gain, in_weight, out_weight.T, table)
    mixed = pl.pallas_call(
        functools.partial(kernel, z),
        out_shape=jax.ShapeDtypeStruct((local, width), BF16),
        in_specs=[hbm] * 5,
        out_specs=vmem,
        scratch_shapes=scratch,
        compiler_params=pltpu.CompilerParams(
            collective_id=0, has_side_effects=True, vmem_limit_bytes=VMEM_LIMIT
        ),
        name="fourier_mix",
    )(*(pltpu.with_memory_space_constraint(a, pltpu.HBM) for a in operands))
    return mixed[None]


def solution(mesh):
    rows, cols = mesh.shape["row"], mesh.shape["col"]
    in_specs = (P("col", "row", None), P(), P("row", "col"), P("col", "row"))
    return jax.shard_map(
        functools.partial(body, rows, cols), mesh=mesh, in_specs=in_specs,
        out_specs=P("col", "row", None), check_vma=False,
    )
```

```python
import functools
import math

import jax
import jax.numpy as jnp
import numpy as np
from jax import lax
from jax.experimental import pallas as pl
from jax.experimental.pallas import tpu as pltpu
from jax.sharding import PartitionSpec as P

GS = 64
HALF = GS // 2
EPS = 1e-06
F32 = jnp.float32
BF16 = jnp.bfloat16
MESH = pl.DeviceIdType.MESH
VMEM_LIMIT = 52 * 1024 * 1024


class Sizes:
    def __init__(self, rows, cols, local, width):
        self.rows = rows
        self.nz = 1 << ((rows.bit_length() - 1 + 1) // 2)
        self.ny = rows // self.nz
        self.nx = cols // 2
        self.local = local
        self.width = width
        self.ch = GS * self.nx
        self.per = 2 * self.ch // rows
        self.pairs = self.per // 2
        self.hops = local // rows
        self.blk = width // rows
        self.cut = 4
        self.tiles = max(1, local // 128)
        self.lane = local // self.tiles


def tables(z):
    rows, local, ch = z.rows, z.local, z.ch
    length = rows * local
    k = np.arange(GS)
    small = np.zeros((GS, GS))
    for j in range(HALF):
        if j == 0:
            small[0] = (1.0 + (-1.0) ** k) / 2
            small[1] = (1.0 - (-1.0) ** k) / 2
        else:
            small[2 * j] = np.cos(2 * math.pi * j * k / GS)
            small[2 * j + 1] = np.sin(2 * math.pi * j * k / GS)
    chan = np.kron(np.eye(z.nx), small)
    i = np.arange(rows)
    ang = 2 * math.pi * (np.outer(i, i) % rows) / rows
    c, s = np.cos(ang), np.sin(ang)
    first = np.concatenate(
        [
            np.block([[c, -s], [-s, -c], [c, s], [-s, c]]),
            np.block([[c, c], [-s, -s], [c, -c], [-s, s]]),
        ]
    )
    m = np.arange(local)
    tw = 2 * math.pi * np.outer(i, m) / length
    turn = np.concatenate([np.cos(tw), np.sin(tw)]).astype(np.float32)
    high = turn.astype(BF16).astype(np.float32)
    turn = np.concatenate([high, turn - high], axis=1)
    a = np.arange(z.hops)
    k2 = (z.hops * i[None, :] + a[:, None]).reshape(-1)
    ang2 = 2 * math.pi * (np.outer(k2, m) % local) / local
    second = np.concatenate([np.cos(ang2), np.sin(ang2)], axis=1) / math.sqrt(length * GS)
    parts = []
    for part in (second, first, chan, turn):
        wide = np.zeros((part.shape[0], 2 * local), np.float32)
        wide[:, : part.shape[1]] = part
        parts.append(wide)
    return jnp.asarray(np.concatenate(parts).astype(BF16))


def dot(a, b):
    return jnp.dot(a, b, preferred_element_type=F32)


def dot_nt(a, b):
    return lax.dot_general(a, b, (((1,), (1,)), ((), ())), preferred_element_type=F32)


def placed(rows, cols, target, keep):
    to = lax.broadcasted_iota(jnp.int32, (rows, cols), 1)
    return jnp.where((to == target) & keep, 1.0, 0.0).astype(BF16)


def kernel(
    z,
    tok_hbm, gain_hbm, wi_hbm, wt_hbm, tab_hbm,
    out,
    gain_ref, wi_ref, wt_ref, tab, tok,
    xbuf, win, wpk, wo, spread, ht, got, stage, gp, back, got2,
    tab_sem, tok_sem, swap_send, swap_recv,
    x_send, x_recv, in_send, in_recv, ring_recv, wo_send, wo_recv,
    far_send, far_recv, half_send, half_recv,
    a_send, a_recv, b_send, b_recv, plane_sem,
):
    rows, ny, nz, nx, local = z.rows, z.ny, z.nz, z.nx, z.local
    groups = rows // 2
    r = lax.axis_index("row")
    c = lax.axis_index("col")
    h = lax.rem(c, 2)
    x = c // 2
    zz = r // ny
    yy = lax.rem(r, ny)
    other = c + 1 - 2 * h

    def send(src, dst, ssem, rsem, row, col):
        copy = pltpu.make_async_remote_copy(
            src_ref=src, dst_ref=dst, send_sem=ssem, recv_sem=rsem,
            device_id=(row, col), device_id_type=MESH,
        )
        copy.start()

    def drain(ref, sem):
        pltpu.make_async_copy(ref, ref, sem).wait()

    barrier = pltpu.get_barrier_semaphore()
    loads = [
        pltpu.make_async_copy(src, dst, tab_sem.at[n])
        for n, (src, dst) in enumerate(
            [(wi_hbm, wi_ref), (wt_hbm, wt_ref), (gain_hbm, gain_ref), (tab_hbm, tab)]
        )
    ]
    for load in loads[:2]:
        load.start()

    for d in range(1, nx):
        px = lax.rem(x + d, nx)
        pl.semaphore_signal(barrier, inc=1, device_id=(r, 2 * px + h), device_id_type=MESH)
    for d in range(1, ny):
        to = zz * ny + lax.rem(yy + d, ny)
        pl.semaphore_signal(barrier, inc=1, device_id=(to, c), device_id_type=MESH)
    for d in range(1, nz):
        to = lax.rem(zz + d, nz) * ny + yy
        pl.semaphore_signal(barrier, inc=1, device_id=(to, c), device_id_type=MESH)
    pl.semaphore_signal(barrier, inc=1, device_id=(r, other), device_id_type=MESH)

    own = pltpu.make_async_copy(tok_hbm, tok.at[h], tok_sem)
    own.start()
    for load in loads[2:]:
        load.start()
    packed = 2 * GS
    at = lax.broadcasted_iota(jnp.int32, (nx * packed, z.ch), 0)
    for half in range(2):
        q = lax.rem(at, packed) - GS * half
        place = jnp.where(q < HALF, 2 * q, 2 * GS + 1 - 2 * q)
        place = jnp.where(q == HALF, 1, place) + GS * (at // packed)
        spread[half] = placed(nx * packed, z.ch, place, (q >= 0) & (q < GS))
    loads[0].wait()
    loads[1].wait()
    hb = z.blk // 2
    lo, hi = pl.ds(0, hb), pl.ds(hb, hb)
    side = lax.broadcasted_iota(jnp.int32, (GS, packed), 0)
    everywhere = side >= 0
    wpk[h, x, zz, yy] = (
        dot(wt_ref[:hb], placed(GS, packed, side, everywhere))
        + dot(wt_ref[hb:], placed(GS, packed, side + GS, everywhere))
    ).astype(BF16)
    xbuf[x] = wi_ref[...]
    pl.semaphore_wait(barrier, nx + ny + nz - 2)

    for d in range(1, nx):
        px = lax.rem(x + d, nx)
        send(wi_ref, xbuf.at[x], x_send, x_recv, r, 2 * px + h)
    send(tok_hbm, tok.at[h], swap_send, swap_recv, r, other)
    mine = wpk.at[h, x]

    @pl.when(h == 0)
    def _():
        for d in range(1, ny):
            py = lax.rem(yy + d, ny)
            send(mine.at[zz, yy], mine.at[zz, yy], wo_send.at[0], wo_recv.at[0], zz * ny + py, c)

    @pl.when(h == 1)
    def _():
        for d in range(1, nz):
            pz = lax.rem(zz + d, nz)
            send(mine.at[zz, yy], mine.at[zz, yy], wo_send.at[0], wo_recv.at[0], pz * ny + yy, c)

    chan_at = lax.broadcasted_iota(jnp.int32, (GS, z.ch), 0)
    drain(xbuf.at[pl.ds(0, nx - 1)], x_recv)
    total = dot(xbuf[0], placed(GS, z.ch, chan_at, chan_at >= 0))
    for n in range(1, nx):
        total += dot(xbuf[n], placed(GS, z.ch, chan_at + GS * n, chan_at >= 0))
    win[zz, yy] = total.astype(BF16)

    for d in range(1, ny):
        py = lax.rem(yy + d, ny)
        send(win.at[zz, yy, lo], win.at[zz, yy, lo], in_send.at[0], in_recv.at[0], zz * ny + py, c)
    for d in range(1, nz):
        pz = lax.rem(zz + d, nz)
        send(win.at[zz, yy, hi], win.at[zz, yy, hi], in_send.at[1], in_recv.at[1], pz * ny + yy, c)
    loads[2].wait()
    gain = gain_ref[...].astype(F32).reshape(1, z.width)
    step = min(32, local)

    def norm(q):
        def one(i, carry):
            part = pl.ds(pl.multiple_of(i * step, step), step)
            v = tok[q, part, :].astype(F32)
            inv = lax.rsqrt(jnp.mean(v * v, axis=-1, keepdims=True) + EPS)
            tok[q, part, :] = (v * inv * gain).astype(BF16)
            return carry

        lax.fori_loop(0, local // step, one, 0)

    own.wait()
    norm(h)

    drain(win.at[0, pl.ds(0, ny - 1), lo], in_recv.at[0])
    drain(win.at[pl.ds(0, nz - 1), 0, hi], in_recv.at[1])
    cy, cz = min(z.cut, ny), min(z.cut, nz)

    def low(block, chunk):
        return win.at[block, pl.ds(chunk * (ny // cy), ny // cy), lo]

    def high(block, chunk):
        return win.at[pl.ds(chunk * (nz // cz), nz // cz), block, hi]

    def row_z(p):
        return p * ny + yy

    def row_y(p):
        return zz * ny + p

    paths = ((low, nz, zz, cy, row_z), (high, ny, yy, cz, row_y))

    def carried(n, cut, hop, sign):
        if hop < n // 2:
            return range(cut)
        return range(cut // 2) if sign > 0 else range(cut // 2, cut)

    longest = max(nz, ny) // 2

    def advance(hop):
        for chunk in range(max(cy, cz)):
            for p, (view, n, pos, cut, row) in enumerate(paths):
                for e, sign in enumerate((1, -1)):
                    block = lax.rem(pos - sign * (hop - 1) + n, n)
                    if 1 < hop <= n // 2 + 1 and chunk in carried(n, cut, hop - 1, sign):
                        drain(view(block, chunk), ring_recv.at[p, e, hop - 2, chunk])
                    if hop <= n // 2 and chunk in carried(n, cut, hop, sign):
                        to = lax.rem(pos + sign + n, n)
                        send(view(block, chunk), view(block, chunk), in_send.at[2 + p],
                             ring_recv.at[p, e, hop - 1, chunk], row(to), c)

    advance(1)

    @pl.when(h == 0)
    def _():
        drain(wpk.at[0, 0, 0, pl.ds(0, ny - 1)], wo_recv.at[0])
        for d in range(1, nz):
            pz = lax.rem(zz + d, nz)
            send(mine.at[zz], mine.at[zz], wo_send.at[1], wo_recv.at[1], pz * ny + yy, c)

    @pl.when(h == 1)
    def _():
        drain(wpk.at[0, 0, pl.ds(0, nz - 1), 0], wo_recv.at[0])
        for d in range(1, ny):
            py = lax.rem(yy + d, ny)
            send(mine.at[:, yy], mine.at[:, yy], wo_send.at[1], wo_recv.at[1], zz * ny + py, c)

    drain(tok.at[0], swap_recv)
    norm(1 - h)
    for hop in range(2, longest + 2):
        with jax.named_scope(f"pring{hop}"):
            advance(hop)

    pl.semaphore_signal(plane_sem, inc=1, device_id=(r, other), device_id_type=MESH)

    @pl.when(h == 0)
    def _():
        drain(wpk.at[0, 0, pl.ds(0, nz - 1)], wo_recv.at[1])

    @pl.when(h == 1)
    def _():
        drain(wpk.at[0, 0, :, pl.ds(0, ny - 1)], wo_recv.at[1])

    near = (1, nx - 1) if nx == 4 else tuple(range(1, nx))
    for n, d in enumerate(near):
        px = lax.rem(x + d, nx)
        send(mine, mine, far_send, far_recv.at[n], r, 2 * px + h)
    send(mine, mine, half_send, half_recv.at[0], r, other)

    loads[3].wait()
    o1 = local
    o2 = o1 + 8 * rows
    o3 = o2 + z.ch
    chan = tab[o2:o3, :z.ch]
    weight = win[...].reshape(z.width, z.ch)
    for q in range(2):
        proj = dot(tok[q], weight).astype(BF16)
        cols = dot_nt(chan, proj).astype(BF16)
        ht[pl.ds(groups * q, groups)] = cols.reshape(groups, z.per, local)

        def scatter(i, carry):
            peer = groups * q + lax.rem(r + i, groups)

            @pl.when(peer != r)
            def _():
                send(ht.at[peer], got.at[r], a_send, a_recv, peer, c)

            return carry

        lax.fori_loop(0, groups, scatter, 0)
    got[r] = ht[r]

    zh = nz // 2
    for n, d in enumerate(near):
        theirs = wpk.at[h, lax.rem(x - d + nx, nx)]
        drain(theirs, far_recv.at[n])
        if nx == 4:
            part = pl.ds(n * zh, zh)
            to = lax.rem(x + d, nx)
            send(theirs.at[part], theirs.at[part], far_send, far_recv.at[2 + n], r, 2 * to + h)
        send(theirs, theirs, half_send, half_recv.at[1 + n], r, other)

    drain(got.at[pl.ds(0, rows - 1)], a_recv)

    if nx == 4:
        far = lax.rem(x + 2, nx)
        for n in range(2):
            part = wpk.at[h, far, pl.ds(n * zh, zh)]
            drain(part, far_recv.at[2 + n])
            send(part, part, half_send, half_recv.at[3], r, other)

    lane = z.lane
    for l in range(z.tiles):
        part = got[:, :, l * lane:(l + 1) * lane].astype(F32)
        stage[l] = part.reshape(rows * z.per, lane)
    base = lax.rem(r, groups) * z.pairs
    plain = tab[o1:o1 + 4 * rows, :2 * rows]
    for p in range(z.pairs):
        matrix = plain
        if p % min(z.pairs, HALF) == 0:
            paired = tab[o1 + 4 * rows:o2, :2 * rows].astype(F32)
            special = lax.rem(base + p, HALF) == 0
            matrix = jnp.where(special, paired, plain.astype(F32)).astype(BF16)
        for l in range(z.tiles):
            lanes = slice(l * lane, (l + 1) * lane)
            rest = slice(local + l * lane, local + (l + 1) * lane)
            cos = tab[o3:o3 + rows, lanes].astype(F32) + tab[o3:o3 + rows, rest].astype(F32)
            sin = (tab[o3 + rows:o3 + 2 * rows, lanes].astype(F32)
                   + tab[o3 + rows:o3 + 2 * rows, rest].astype(F32))
            u = stage[l, pl.ds(2 * p, rows, stride=z.per), :]
            v = stage[l, pl.ds(2 * p + 1, rows, stride=z.per), :]
            g = dot(matrix, jnp.concatenate([u, v], axis=0).astype(BF16))
            for w in range(2):
                re = g[2 * w * rows:(2 * w + 1) * rows]
                im = g[(2 * w + 1) * rows:(2 * w + 2) * rows]
                at = pl.ds((2 * p + w) * rows, rows)
                gp[at, lanes] = (re * cos + im * sin).astype(BF16)
                gp[at, rest] = (im * cos - re * sin).astype(BF16)
    spec = dot_nt(tab[:local], gp[...])
    if rows == GS and lane == 128:
        left = lax.broadcasted_iota(jnp.int32, (rows, lane), 1) < rows
        for l in range(z.tiles):
            for p in range(z.pairs):
                t0 = spec[2 * l * rows:(2 * l + 1) * rows, p * lane:(p + 1) * lane]
                t1 = spec[(2 * l + 1) * rows:(2 * l + 2) * rows, p * lane:(p + 1) * lane]
                stage[l, pl.ds(2 * p, rows, stride=z.per), :] = jnp.where(
                    left, t0, pltpu.roll(t1, rows, 1)
                )
                stage[l, pl.ds(2 * p + 1, rows, stride=z.per), :] = jnp.where(
                    left, pltpu.roll(t0, rows, 1), t1
                )
    else:
        full = spec.reshape(z.hops, rows, z.per, rows).transpose(1, 2, 0, 3)
        full = full.reshape(rows * z.per, z.tiles, lane)
        for l in range(z.tiles):
            stage[l] = full[:, l]
    for l in range(z.tiles):
        back[:, :, l * lane:(l + 1) * lane] = stage[l].reshape(rows, z.per, lane).astype(BF16)

    pl.semaphore_wait(plane_sem, 1)
    seq = r // groups
    slot = h * groups + lax.rem(r, groups)
    target = 2 * x + seq

    def give(i, carry):
        peer = lax.rem(r + i, rows)
        send(back.at[peer], got2.at[slot], b_send, b_recv, peer, target)
        return carry

    lax.fori_loop(1, rows, give, 0)

    @pl.when(seq == h)
    def _():
        got2[slot] = back[r]

    @pl.when(seq != h)
    def _():
        send(back.at[r], got2.at[slot], b_send, b_recv, r, target)

    def unpack(half_of):
        flat = jnp.concatenate(
            [wpk[half_of, n].reshape(rows * hb, packed) for n in range(nx)], axis=1
        )
        for half in range(2):
            sorted_ = dot(flat, spread[half]).astype(BF16)
            wo[half_of, :, half * hb:(half + 1) * hb, :] = sorted_.reshape(rows, hb, z.ch)

    unpack(h)
    for n in range(nx):
        drain(wpk.at[0, 0], half_recv.at[n])
    unpack(1 - h)

    @pl.when(seq == h)
    def _():
        drain(got2.at[pl.ds(0, rows - 1)], b_recv)

    @pl.when(seq != h)
    def _():
        drain(got2, b_recv)

    mixed = got2[...].astype(F32).reshape(rows * z.per, local).T.astype(BF16)
    ma, mb = mixed[:, :z.ch], mixed[:, z.ch:]
    chunk = ny * z.blk
    for n in range(nz):
        some = pl.ds(n * ny, ny)
        res = dot_nt(ma, wo[0, some].reshape(chunk, z.ch)) + dot_nt(mb, wo[1, some].reshape(chunk, z.ch))
        out[:, n * chunk:(n + 1) * chunk] = res.astype(BF16)

    drain(xbuf.at[pl.ds(0, nx - 1)], x_send)
    drain(tok.at[0], swap_send)
    drain(win.at[0, pl.ds(0, ny - 1), lo], in_send.at[0])
    drain(win.at[pl.ds(0, nz - 1), 0, hi], in_send.at[1])
    drain(win.at[pl.ds(0, nz - 1), :, lo], in_send.at[2])
    drain(win.at[:, pl.ds(0, ny - 1), hi], in_send.at[3])

    @pl.when(h == 0)
    def _():
        drain(wpk.at[0, 0, 0, pl.ds(0, ny - 1)], wo_send.at[0])
        drain(wpk.at[0, 0, pl.ds(0, nz - 1)], wo_send.at[1])

    @pl.when(h == 1)
    def _():
        drain(wpk.at[0, 0, pl.ds(0, nz - 1), 0], wo_send.at[0])
        drain(wpk.at[0, 0, :, pl.ds(0, ny - 1)], wo_send.at[1])

    drain(wpk.at[0, pl.ds(0, nx - 1)], far_send)
    drain(wpk.at[0], half_send)
    drain(ht.at[pl.ds(0, rows - 1)], a_send)

    @pl.when(seq == h)
    def _():
        drain(back.at[pl.ds(0, rows - 1)], b_send)

    @pl.when(seq != h)
    def _():
        drain(back, b_send)


def body(rows, cols, tokens, norm_gain, in_weight, out_weight):
    local, width = tokens.shape[1:]
    z = Sizes(rows, cols, local, width)
    table = tables(z)
    hbm = pl.BlockSpec(memory_space=pltpu.HBM)
    vmem = pl.BlockSpec(memory_space=pltpu.VMEM)
    hb = z.blk // 2
    dma = pltpu.SemaphoreType.DMA
    vm = pltpu.VMEM
    exchange = (rows, z.per, local)
    scratch = [
        vm((width,), BF16),
        vm((z.blk, GS), BF16),
        vm((z.blk, GS), BF16),
        vm(table.shape, BF16),
        vm((2, local, width), BF16),
        vm((z.nx, z.blk, GS), BF16),
        vm((z.nz, z.ny, z.blk, z.ch), BF16),
        vm((2, z.nx, z.nz, z.ny, hb, 2 * GS), BF16),
        vm((2, rows, z.blk, z.ch), BF16),
        vm((2, 2 * GS * z.nx, z.ch), BF16),
        vm(exchange, BF16),
        vm(exchange, BF16),
        vm((z.tiles, rows * z.per, z.lane), F32),
        vm((z.per * rows, 2 * local), BF16),
        vm(exchange, BF16),
        vm(exchange, BF16),
        dma((4,)), dma, dma, dma,
        dma, dma, dma((4,)), dma((2,)), dma((2, 2, max(z.ny, z.nz) // 2, z.cut)), dma((2,)), dma((2,)),
        dma, dma((4,)), dma, dma((4,)),
        dma, dma, dma, dma, pltpu.SemaphoreType.REGULAR,
    ]
    operands = (tokens[0], norm_gain, in_weight, out_weight.T, table)
    mixed = pl.pallas_call(
        functools.partial(kernel, z),
        out_shape=jax.ShapeDtypeStruct((local, width), BF16),
        in_specs=[hbm] * 5,
        out_specs=vmem,
        scratch_shapes=scratch,
        compiler_params=pltpu.CompilerParams(
            collective_id=0, has_side_effects=True, vmem_limit_bytes=VMEM_LIMIT
        ),
        name="fourier_mix",
    )(*(pltpu.with_memory_space_constraint(a, pltpu.HBM) for a in operands))
    return mixed[None]


def solution(mesh):
    rows, cols = mesh.shape["row"], mesh.shape["col"]
    in_specs = (P("col", "row", None), P(), P("row", "col"), P("col", "row"))
    return jax.shard_map(
        functools.partial(body, rows, cols), mesh=mesh, in_specs=in_specs,
        out_specs=P("col", "row", None), check_vma=False,
    )
```

```python
import functools
import math

import jax
import jax.numpy as jnp
import numpy as np
from jax import lax
from jax.experimental import pallas as pl
from jax.experimental.pallas import tpu as pltpu
from jax.sharding import PartitionSpec as P

GS = 64
HALF = GS // 2
EPS = 1e-06
F32 = jnp.float32
BF16 = jnp.bfloat16
MESH = pl.DeviceIdType.MESH
VMEM_LIMIT = 52 * 1024 * 1024


class Sizes:
    def __init__(self, rows, cols, local, width):
        self.rows = rows
        self.nz = 1 << ((rows.bit_length() - 1 + 1) // 2)
        self.ny = rows // self.nz
        self.nx = cols // 2
        self.local = local
        self.width = width
        self.ch = GS * self.nx
        self.per = 2 * self.ch // rows
        self.pairs = self.per // 2
        self.hops = local // rows
        self.blk = width // rows
        self.cut = 4
        self.tiles = max(1, local // 128)
        self.lane = local // self.tiles


def tables(z):
    rows, local, ch = z.rows, z.local, z.ch
    length = rows * local
    k = np.arange(GS)
    small = np.zeros((GS, GS))
    for j in range(HALF):
        if j == 0:
            small[0] = (1.0 + (-1.0) ** k) / 2
            small[1] = (1.0 - (-1.0) ** k) / 2
        else:
            small[2 * j] = np.cos(2 * math.pi * j * k / GS)
            small[2 * j + 1] = np.sin(2 * math.pi * j * k / GS)
    chan = np.kron(np.eye(z.nx), small)
    i = np.arange(rows)
    ang = 2 * math.pi * (np.outer(i, i) % rows) / rows
    c, s = np.cos(ang), np.sin(ang)
    first = np.concatenate(
        [
            np.block([[c, -s], [-s, -c], [c, s], [-s, c]]),
            np.block([[c, c], [-s, -s], [c, -c], [-s, s]]),
        ]
    )
    m = np.arange(local)
    tw = 2 * math.pi * np.outer(i, m) / length
    turn = np.concatenate([np.cos(tw), np.sin(tw)]).astype(np.float32)
    high = turn.astype(BF16).astype(np.float32)
    turn = np.concatenate([high, turn - high], axis=1)
    a = np.arange(z.hops)
    k2 = (z.hops * i[None, :] + a[:, None]).reshape(-1)
    ang2 = 2 * math.pi * (np.outer(k2, m) % local) / local
    second = np.concatenate([np.cos(ang2), np.sin(ang2)], axis=1) / math.sqrt(length * GS)
    parts = []
    for part in (second, first, chan, turn):
        wide = np.zeros((part.shape[0], 2 * local), np.float32)
        wide[:, : part.shape[1]] = part
        parts.append(wide)
    return jnp.asarray(np.concatenate(parts).astype(BF16))


def dot(a, b):
    return jnp.dot(a, b, preferred_element_type=F32)


def dot_nt(a, b):
    return lax.dot_general(a, b, (((1,), (1,)), ((), ())), preferred_element_type=F32)


def placed(rows, cols, target, keep):
    to = lax.broadcasted_iota(jnp.int32, (rows, cols), 1)
    return jnp.where((to == target) & keep, 1.0, 0.0).astype(BF16)


def kernel(
    z,
    tok_hbm, gain_hbm, wi_hbm, wt_hbm, tab_hbm,
    out,
    gain_ref, wi_ref, wt_ref, tab, tok,
    xbuf, win, wpk, wo, spread, ht, got, stage, gp, back, got2,
    tab_sem, tok_sem, swap_send, swap_recv,
    x_send, x_recv, in_send, in_recv, ring_recv, wo_send, wo_recv,
    far_send, far_recv, half_send, half_recv,
    a_send, a_recv, b_send, b_recv, plane_sem,
):
    rows, ny, nz, nx, local = z.rows, z.ny, z.nz, z.nx, z.local
    groups = rows // 2
    r = lax.axis_index("row")
    c = lax.axis_index("col")
    h = lax.rem(c, 2)
    x = c // 2
    zz = r // ny
    yy = lax.rem(r, ny)
    other = c + 1 - 2 * h

    def send(src, dst, ssem, rsem, row, col):
        copy = pltpu.make_async_remote_copy(
            src_ref=src, dst_ref=dst, send_sem=ssem, recv_sem=rsem,
            device_id=(row, col), device_id_type=MESH,
        )
        copy.start()

    def drain(ref, sem):
        pltpu.make_async_copy(ref, ref, sem).wait()

    barrier = pltpu.get_barrier_semaphore()
    loads = [
        pltpu.make_async_copy(src, dst, tab_sem.at[n])
        for n, (src, dst) in enumerate(
            [(wi_hbm, wi_ref), (wt_hbm, wt_ref), (gain_hbm, gain_ref), (tab_hbm, tab)]
        )
    ]
    for load in loads[:2]:
        load.start()

    for d in range(1, nx):
        px = lax.rem(x + d, nx)
        pl.semaphore_signal(barrier, inc=1, device_id=(r, 2 * px + h), device_id_type=MESH)
    for d in range(1, ny):
        to = zz * ny + lax.rem(yy + d, ny)
        pl.semaphore_signal(barrier, inc=1, device_id=(to, c), device_id_type=MESH)
    for d in range(1, nz):
        to = lax.rem(zz + d, nz) * ny + yy
        pl.semaphore_signal(barrier, inc=1, device_id=(to, c), device_id_type=MESH)
    pl.semaphore_signal(barrier, inc=1, device_id=(r, other), device_id_type=MESH)

    own = pltpu.make_async_copy(tok_hbm, tok.at[h], tok_sem)
    own.start()
    for load in loads[2:]:
        load.start()
    packed = 2 * GS
    at = lax.broadcasted_iota(jnp.int32, (nx * packed, z.ch), 0)
    for half in range(2):
        q = lax.rem(at, packed) - GS * half
        place = jnp.where(q < HALF, 2 * q, 2 * GS + 1 - 2 * q)
        place = jnp.where(q == HALF, 1, place) + GS * (at // packed)
        spread[half] = placed(nx * packed, z.ch, place, (q >= 0) & (q < GS))
    loads[0].wait()
    loads[1].wait()
    hb = z.blk // 2
    lo, hi = pl.ds(0, hb), pl.ds(hb, hb)
    side = lax.broadcasted_iota(jnp.int32, (GS, packed), 0)
    everywhere = side >= 0
    wpk[h, x, zz, yy] = (
        dot(wt_ref[:hb], placed(GS, packed, side, everywhere))
        + dot(wt_ref[hb:], placed(GS, packed, side + GS, everywhere))
    ).astype(BF16)
    xbuf[x] = wi_ref[...]
    pl.semaphore_wait(barrier, nx + ny + nz - 2)

    for d in range(1, nx):
        px = lax.rem(x + d, nx)
        send(wi_ref, xbuf.at[x], x_send, x_recv, r, 2 * px + h)
    send(tok_hbm, tok.at[h], swap_send, swap_recv, r, other)
    mine = wpk.at[h, x]

    @pl.when(h == 0)
    def _():
        for d in range(1, ny):
            py = lax.rem(yy + d, ny)
            send(mine.at[zz, yy], mine.at[zz, yy], wo_send.at[0], wo_recv.at[0], zz * ny + py, c)

    @pl.when(h == 1)
    def _():
        for d in range(1, nz):
            pz = lax.rem(zz + d, nz)
            send(mine.at[zz, yy], mine.at[zz, yy], wo_send.at[0], wo_recv.at[0], pz * ny + yy, c)

    chan_at = lax.broadcasted_iota(jnp.int32, (GS, z.ch), 0)
    drain(xbuf.at[pl.ds(0, nx - 1)], x_recv)
    total = dot(xbuf[0], placed(GS, z.ch, chan_at, chan_at >= 0))
    for n in range(1, nx):
        total += dot(xbuf[n], placed(GS, z.ch, chan_at + GS * n, chan_at >= 0))
    win[zz, yy] = total.astype(BF16)

    for d in range(1, ny):
        py = lax.rem(yy + d, ny)
        send(win.at[zz, yy, lo], win.at[zz, yy, lo], in_send.at[0], in_recv.at[0], zz * ny + py, c)
    for d in range(1, nz):
        pz = lax.rem(zz + d, nz)
        send(win.at[zz, yy, hi], win.at[zz, yy, hi], in_send.at[1], in_recv.at[1], pz * ny + yy, c)
    loads[2].wait()
    gain = gain_ref[...].astype(F32).reshape(1, z.width)
    step = min(32, local)

    def norm(q):
        def one(i, carry):
            part = pl.ds(pl.multiple_of(i * step, step), step)
            v = tok[q, part, :].astype(F32)
            inv = lax.rsqrt(jnp.mean(v * v, axis=-1, keepdims=True) + EPS)
            tok[q, part, :] = (v * inv * gain).astype(BF16)
            return carry

        lax.fori_loop(0, local // step, one, 0)

    own.wait()
    norm(h)

    @pl.when(h == 0)
    def _():
        drain(wpk.at[0, 0, 0, pl.ds(0, ny - 1)], wo_recv.at[0])
        for d in range(1, nz):
            pz = lax.rem(zz + d, nz)
            send(mine.at[zz], mine.at[zz], wo_send.at[1], wo_recv.at[1], pz * ny + yy, c)

    @pl.when(h == 1)
    def _():
        drain(wpk.at[0, 0, pl.ds(0, nz - 1), 0], wo_recv.at[0])
        for d in range(1, ny):
            py = lax.rem(yy + d, ny)
            send(mine.at[:, yy], mine.at[:, yy], wo_send.at[1], wo_recv.at[1], zz * ny + py, c)

    drain(win.at[0, pl.ds(0, ny - 1), lo], in_recv.at[0])
    drain(win.at[pl.ds(0, nz - 1), 0, hi], in_recv.at[1])
    cy, cz = min(z.cut, ny), min(z.cut, nz)

    def low(block, chunk):
        return win.at[block, pl.ds(chunk * (ny // cy), ny // cy), lo]

    def high(block, chunk):
        return win.at[pl.ds(chunk * (nz // cz), nz // cz), block, hi]

    def row_z(p):
        return p * ny + yy

    def row_y(p):
        return zz * ny + p

    paths = ((low, nz, zz, cy, row_z), (high, ny, yy, cz, row_y))

    def carried(n, cut, hop, sign):
        if hop < n // 2:
            return range(cut)
        return range(cut // 2) if sign > 0 else range(cut // 2, cut)

    longest = max(nz, ny) // 2
    line8 = nz == 8 and ny == 8

    def hand(view, chunk, block, p, e, kind, to, row):
        send(view(block, chunk), view(block, chunk), in_send.at[2 + p],
             ring_recv.at[p, e, kind, chunk], row(to), c)

    def start8():
        for chunk in range(z.cut):
            for far in (2, 1):
                for p, (view, n, pos, cut, row) in enumerate(paths):
                    for e, sign in enumerate((1, -1)):
                        hand(view, chunk, pos, p, e, far - 1, lax.rem(pos + far * sign + n, n), row)

    def relay8():
        for chunk in range(z.cut):
            for p, (view, n, pos, cut, row) in enumerate(paths):
                for e, sign in enumerate((1, -1)):
                    block = lax.rem(pos - 2 * sign + n, n)
                    drain(view(block, chunk), ring_recv.at[p, e, 1, chunk])
                    hand(view, chunk, block, p, e, 2, lax.rem(pos + sign + n, n), row)
                    if chunk in carried(n, cut, n // 2, sign):
                        hand(view, chunk, block, p, e, 3, lax.rem(pos + 2 * sign + n, n), row)

    def finish8():
        for kind in (0, 2, 3):
            for chunk in range(z.cut):
                for p, (view, n, pos, cut, row) in enumerate(paths):
                    for e, sign in enumerate((1, -1)):
                        if kind < 3 or chunk in carried(n, cut, n // 2, sign):
                            drain(view(pos, chunk), ring_recv.at[p, e, kind, chunk])

    def advance(hop):
        for chunk in range(max(cy, cz)):
            for p, (view, n, pos, cut, row) in enumerate(paths):
                for e, sign in enumerate((1, -1)):
                    block = lax.rem(pos - sign * (hop - 1) + n, n)
                    if 1 < hop <= n // 2 + 1 and chunk in carried(n, cut, hop - 1, sign):
                        drain(view(block, chunk), ring_recv.at[p, e, hop - 2, chunk])
                    if hop <= n // 2 and chunk in carried(n, cut, hop, sign):
                        to = lax.rem(pos + sign + n, n)
                        send(view(block, chunk), view(block, chunk), in_send.at[2 + p],
                             ring_recv.at[p, e, hop - 1, chunk], row(to), c)

    if line8:
        start8()
    else:
        advance(1)

    drain(tok.at[0], swap_recv)
    norm(1 - h)
    if line8:
        with jax.named_scope("pring2"):
            relay8()
        with jax.named_scope("pring3"):
            finish8()
    else:
        for hop in range(2, longest + 2):
            advance(hop)

    pl.semaphore_signal(plane_sem, inc=1, device_id=(r, other), device_id_type=MESH)

    @pl.when(h == 0)
    def _():
        drain(wpk.at[0, 0, pl.ds(0, nz - 1)], wo_recv.at[1])

    @pl.when(h == 1)
    def _():
        drain(wpk.at[0, 0, :, pl.ds(0, ny - 1)], wo_recv.at[1])

    near = (1, nx - 1) if nx == 4 else tuple(range(1, nx))
    for n, d in enumerate(near):
        px = lax.rem(x + d, nx)
        send(mine, mine, far_send, far_recv.at[n], r, 2 * px + h)
    send(mine, mine, half_send, half_recv.at[0], r, other)

    loads[3].wait()
    o1 = local
    o2 = o1 + 8 * rows
    o3 = o2 + z.ch
    chan = tab[o2:o3, :z.ch]
    weight = win[...].reshape(z.width, z.ch)
    for q in range(2):
        proj = dot(tok[q], weight).astype(BF16)
        cols = dot_nt(chan, proj).astype(BF16)
        ht[pl.ds(groups * q, groups)] = cols.reshape(groups, z.per, local)

        def scatter(i, carry):
            peer = groups * q + lax.rem(r + i, groups)

            @pl.when(peer != r)
            def _():
                send(ht.at[peer], got.at[r], a_send, a_recv, peer, c)

            return carry

        lax.fori_loop(0, groups, scatter, 0)
    got[r] = ht[r]

    zh = nz // 2
    for n, d in enumerate(near):
        theirs = wpk.at[h, lax.rem(x - d + nx, nx)]
        drain(theirs, far_recv.at[n])
        if nx == 4:
            part = pl.ds(n * zh, zh)
            to = lax.rem(x + d, nx)
            send(theirs.at[part], theirs.at[part], far_send, far_recv.at[2 + n], r, 2 * to + h)
        send(theirs, theirs, half_send, half_recv.at[1 + n], r, other)

    drain(got.at[pl.ds(0, rows - 1)], a_recv)

    if nx == 4:
        far = lax.rem(x + 2, nx)
        for n in range(2):
            part = wpk.at[h, far, pl.ds(n * zh, zh)]
            drain(part, far_recv.at[2 + n])
            send(part, part, half_send, half_recv.at[3], r, other)

    lane = z.lane
    for l in range(z.tiles):
        part = got[:, :, l * lane:(l + 1) * lane].astype(F32)
        stage[l] = part.reshape(rows * z.per, lane)
    base = lax.rem(r, groups) * z.pairs
    plain = tab[o1:o1 + 4 * rows, :2 * rows]
    for p in range(z.pairs):
        matrix = plain
        if p % min(z.pairs, HALF) == 0:
            paired = tab[o1 + 4 * rows:o2, :2 * rows].astype(F32)
            special = lax.rem(base + p, HALF) == 0
            matrix = jnp.where(special, paired, plain.astype(F32)).astype(BF16)
        for l in range(z.tiles):
            lanes = slice(l * lane, (l + 1) * lane)
            rest = slice(local + l * lane, local + (l + 1) * lane)
            cos = tab[o3:o3 + rows, lanes].astype(F32) + tab[o3:o3 + rows, rest].astype(F32)
            sin = (tab[o3 + rows:o3 + 2 * rows, lanes].astype(F32)
                   + tab[o3 + rows:o3 + 2 * rows, rest].astype(F32))
            u = stage[l, pl.ds(2 * p, rows, stride=z.per), :]
            v = stage[l, pl.ds(2 * p + 1, rows, stride=z.per), :]
            g = dot(matrix, jnp.concatenate([u, v], axis=0).astype(BF16))
            for w in range(2):
                re = g[2 * w * rows:(2 * w + 1) * rows]
                im = g[(2 * w + 1) * rows:(2 * w + 2) * rows]
                at = pl.ds((2 * p + w) * rows, rows)
                gp[at, lanes] = (re * cos + im * sin).astype(BF16)
                gp[at, rest] = (im * cos - re * sin).astype(BF16)
    spec = dot_nt(tab[:local], gp[...])
    if rows == GS and lane == 128:
        left = lax.broadcasted_iota(jnp.int32, (rows, lane), 1) < rows
        for l in range(z.tiles):
            for p in range(z.pairs):
                t0 = spec[2 * l * rows:(2 * l + 1) * rows, p * lane:(p + 1) * lane]
                t1 = spec[(2 * l + 1) * rows:(2 * l + 2) * rows, p * lane:(p + 1) * lane]
                stage[l, pl.ds(2 * p, rows, stride=z.per), :] = jnp.where(
                    left, t0, pltpu.roll(t1, rows, 1)
                )
                stage[l, pl.ds(2 * p + 1, rows, stride=z.per), :] = jnp.where(
                    left, pltpu.roll(t0, rows, 1), t1
                )
    else:
        full = spec.reshape(z.hops, rows, z.per, rows).transpose(1, 2, 0, 3)
        full = full.reshape(rows * z.per, z.tiles, lane)
        for l in range(z.tiles):
            stage[l] = full[:, l]
    for l in range(z.tiles):
        back[:, :, l * lane:(l + 1) * lane] = stage[l].reshape(rows, z.per, lane).astype(BF16)

    pl.semaphore_wait(plane_sem, 1)
    seq = r // groups
    slot = h * groups + lax.rem(r, groups)
    target = 2 * x + seq

    for k in range(nz):
        pz = k // 2 + (k % 2) * (nz // 2)

        def give(i, carry, pz=pz):
            peer = pz * ny + lax.rem(yy + i, ny)
            send(back.at[peer], got2.at[slot], b_send, b_recv, peer, target)
            return carry

        lax.fori_loop(1, ny, give, 0)

        @pl.when(pz != zz)
        def _(pz=pz, give=give):
            give(0, 0)

    @pl.when(seq == h)
    def _():
        got2[slot] = back[r]

    @pl.when(seq != h)
    def _():
        send(back.at[r], got2.at[slot], b_send, b_recv, r, target)

    def unpack(half_of):
        flat = jnp.concatenate(
            [wpk[half_of, n].reshape(rows * hb, packed) for n in range(nx)], axis=1
        )
        for half in range(2):
            sorted_ = dot(flat, spread[half]).astype(BF16)
            wo[half_of, :, half * hb:(half + 1) * hb, :] = sorted_.reshape(rows, hb, z.ch)

    unpack(h)
    for n in range(nx):
        drain(wpk.at[0, 0], half_recv.at[n])
    unpack(1 - h)

    @pl.when(seq == h)
    def _():
        drain(got2.at[pl.ds(0, rows - 1)], b_recv)

    @pl.when(seq != h)
    def _():
        drain(got2, b_recv)

    mixed = got2[...].astype(F32).reshape(rows * z.per, local).T.astype(BF16)
    ma, mb = mixed[:, :z.ch], mixed[:, z.ch:]
    chunk = ny * z.blk
    for n in range(nz):
        some = pl.ds(n * ny, ny)
        res = dot_nt(ma, wo[0, some].reshape(chunk, z.ch)) + dot_nt(mb, wo[1, some].reshape(chunk, z.ch))
        out[:, n * chunk:(n + 1) * chunk] = res.astype(BF16)

    drain(xbuf.at[pl.ds(0, nx - 1)], x_send)
    drain(tok.at[0], swap_send)
    drain(win.at[0, pl.ds(0, ny - 1), lo], in_send.at[0])
    drain(win.at[pl.ds(0, nz - 1), 0, hi], in_send.at[1])
    drain(win.at[pl.ds(0, nz - 1), :, lo], in_send.at[2])
    drain(win.at[:, pl.ds(0, ny - 1), hi], in_send.at[3])

    @pl.when(h == 0)
    def _():
        drain(wpk.at[0, 0, 0, pl.ds(0, ny - 1)], wo_send.at[0])
        drain(wpk.at[0, 0, pl.ds(0, nz - 1)], wo_send.at[1])

    @pl.when(h == 1)
    def _():
        drain(wpk.at[0, 0, pl.ds(0, nz - 1), 0], wo_send.at[0])
        drain(wpk.at[0, 0, :, pl.ds(0, ny - 1)], wo_send.at[1])

    drain(wpk.at[0, pl.ds(0, nx - 1)], far_send)
    drain(wpk.at[0], half_send)
    drain(ht.at[pl.ds(0, rows - 1)], a_send)

    @pl.when(seq == h)
    def _():
        drain(back.at[pl.ds(0, rows - 1)], b_send)

    @pl.when(seq != h)
    def _():
        drain(back, b_send)


def body(rows, cols, tokens, norm_gain, in_weight, out_weight):
    local, width = tokens.shape[1:]
    z = Sizes(rows, cols, local, width)
    table = tables(z)
    hbm = pl.BlockSpec(memory_space=pltpu.HBM)
    vmem = pl.BlockSpec(memory_space=pltpu.VMEM)
    hb = z.blk // 2
    dma = pltpu.SemaphoreType.DMA
    vm = pltpu.VMEM
    exchange = (rows, z.per, local)
    scratch = [
        vm((width,), BF16),
        vm((z.blk, GS), BF16),
        vm((z.blk, GS), BF16),
        vm(table.shape, BF16),
        vm((2, local, width), BF16),
        vm((z.nx, z.blk, GS), BF16),
        vm((z.nz, z.ny, z.blk, z.ch), BF16),
        vm((2, z.nx, z.nz, z.ny, hb, 2 * GS), BF16),
        vm((2, rows, z.blk, z.ch), BF16),
        vm((2, 2 * GS * z.nx, z.ch), BF16),
        vm(exchange, BF16),
        vm(exchange, BF16),
        vm((z.tiles, rows * z.per, z.lane), F32),
        vm((z.per * rows, 2 * local), BF16),
        vm(exchange, BF16),
        vm(exchange, BF16),
        dma((4,)), dma, dma, dma,
        dma, dma, dma((4,)), dma((2,)), dma((2, 2, max(z.ny, z.nz) // 2, z.cut)), dma((2,)), dma((2,)),
        dma, dma((4,)), dma, dma((4,)),
        dma, dma, dma, dma, pltpu.SemaphoreType.REGULAR,
    ]
    operands = (tokens[0], norm_gain, in_weight, out_weight.T, table)
    mixed = pl.pallas_call(
        functools.partial(kernel, z),
        out_shape=jax.ShapeDtypeStruct((local, width), BF16),
        in_specs=[hbm] * 5,
        out_specs=vmem,
        scratch_shapes=scratch,
        compiler_params=pltpu.CompilerParams(
            collective_id=0, has_side_effects=True, vmem_limit_bytes=VMEM_LIMIT
        ),
        name="fourier_mix",
    )(*(pltpu.with_memory_space_constraint(a, pltpu.HBM) for a in operands))
    return mixed[None]


def solution(mesh):
    rows, cols = mesh.shape["row"], mesh.shape["col"]
    in_specs = (P("col", "row", None), P(), P("row", "col"), P("col", "row"))
    return jax.shard_map(
        functools.partial(body, rows, cols), mesh=mesh, in_specs=in_specs,
        out_specs=P("col", "row", None), check_vma=False,
    )
```

```python
import functools
import math

import jax
import jax.numpy as jnp
import numpy as np
from jax import lax
from jax.experimental import pallas as pl
from jax.experimental.pallas import tpu as pltpu
from jax.sharding import PartitionSpec as P

GS = 64
HALF = GS // 2
EPS = 1e-06
F32 = jnp.float32
BF16 = jnp.bfloat16
MESH = pl.DeviceIdType.MESH
VMEM_LIMIT = 52 * 1024 * 1024


class Sizes:
    def __init__(self, rows, cols, local, width):
        self.rows = rows
        self.nz = 1 << ((rows.bit_length() - 1 + 1) // 2)
        self.ny = rows // self.nz
        self.nx = cols // 2
        self.local = local
        self.width = width
        self.ch = GS * self.nx
        self.per = 2 * self.ch // rows
        self.pairs = self.per // 2
        self.hops = local // rows
        self.blk = width // rows
        self.cut = 4
        self.tiles = max(1, local // 128)
        self.lane = local // self.tiles


def tables(z):
    rows, local, ch = z.rows, z.local, z.ch
    length = rows * local
    k = np.arange(GS)
    small = np.zeros((GS, GS))
    for j in range(HALF):
        if j == 0:
            small[0] = (1.0 + (-1.0) ** k) / 2
            small[1] = (1.0 - (-1.0) ** k) / 2
        else:
            small[2 * j] = np.cos(2 * math.pi * j * k / GS)
            small[2 * j + 1] = np.sin(2 * math.pi * j * k / GS)
    chan = np.kron(np.eye(z.nx), small)
    i = np.arange(rows)
    ang = 2 * math.pi * (np.outer(i, i) % rows) / rows
    c, s = np.cos(ang), np.sin(ang)
    first = np.concatenate(
        [
            np.block([[c, -s], [-s, -c], [c, s], [-s, c]]),
            np.block([[c, c], [-s, -s], [c, -c], [-s, s]]),
        ]
    )
    m = np.arange(local)
    tw = 2 * math.pi * np.outer(i, m) / length
    turn = np.concatenate([np.cos(tw), np.sin(tw)]).astype(np.float32)
    high = turn.astype(BF16).astype(np.float32)
    turn = np.concatenate([high, turn - high], axis=1)
    a = np.arange(z.hops)
    k2 = (z.hops * i[None, :] + a[:, None]).reshape(-1)
    ang2 = 2 * math.pi * (np.outer(k2, m) % local) / local
    second = np.concatenate([np.cos(ang2), np.sin(ang2)], axis=1) / math.sqrt(length * GS)
    parts = []
    for part in (second, first, chan, turn):
        wide = np.zeros((part.shape[0], 2 * local), np.float32)
        wide[:, : part.shape[1]] = part
        parts.append(wide)
    return jnp.asarray(np.concatenate(parts).astype(BF16))


def dot(a, b):
    return jnp.dot(a, b, preferred_element_type=F32)


def dot_nt(a, b):
    return lax.dot_general(a, b, (((1,), (1,)), ((), ())), preferred_element_type=F32)


def placed(rows, cols, target, keep):
    to = lax.broadcasted_iota(jnp.int32, (rows, cols), 1)
    return jnp.where((to == target) & keep, 1.0, 0.0).astype(BF16)


def kernel(
    z,
    tok_hbm, gain_hbm, wi_hbm, wt_hbm, tab_hbm,
    out,
    gain_ref, wi_ref, wt_ref, tab, tok,
    xbuf, win, wpk, wo, spread, ht, got, stage, gp, back, got2,
    tab_sem, tok_sem, swap_send, swap_recv,
    x_send, x_recv, in_send, in_recv, ring_recv, wo_send, wo_recv,
    far_send, far_recv, half_send, half_recv,
    a_send, a_recv, b_send, b_recv, plane_sem,
):
    rows, ny, nz, nx, local = z.rows, z.ny, z.nz, z.nx, z.local
    groups = rows // 2
    r = lax.axis_index("row")
    c = lax.axis_index("col")
    h = lax.rem(c, 2)
    x = c // 2
    zz = r // ny
    yy = lax.rem(r, ny)
    other = c + 1 - 2 * h

    def send(src, dst, ssem, rsem, row, col):
        copy = pltpu.make_async_remote_copy(
            src_ref=src, dst_ref=dst, send_sem=ssem, recv_sem=rsem,
            device_id=(row, col), device_id_type=MESH,
        )
        copy.start()

    def drain(ref, sem):
        pltpu.make_async_copy(ref, ref, sem).wait()

    barrier = pltpu.get_barrier_semaphore()
    loads = [
        pltpu.make_async_copy(src, dst, tab_sem.at[n])
        for n, (src, dst) in enumerate(
            [(wi_hbm, wi_ref), (wt_hbm, wt_ref), (gain_hbm, gain_ref), (tab_hbm, tab)]
        )
    ]
    for load in loads[:2]:
        load.start()

    for d in range(1, nx):
        px = lax.rem(x + d, nx)
        pl.semaphore_signal(barrier, inc=1, device_id=(r, 2 * px + h), device_id_type=MESH)
    for d in range(1, ny):
        to = zz * ny + lax.rem(yy + d, ny)
        pl.semaphore_signal(barrier, inc=1, device_id=(to, c), device_id_type=MESH)
    for d in range(1, nz):
        to = lax.rem(zz + d, nz) * ny + yy
        pl.semaphore_signal(barrier, inc=1, device_id=(to, c), device_id_type=MESH)
    pl.semaphore_signal(barrier, inc=1, device_id=(r, other), device_id_type=MESH)

    own = pltpu.make_async_copy(tok_hbm, tok.at[h], tok_sem)
    own.start()
    for load in loads[2:]:
        load.start()
    packed = 2 * GS
    at = lax.broadcasted_iota(jnp.int32, (nx * packed, z.ch), 0)
    for half in range(2):
        q = lax.rem(at, packed) - GS * half
        place = jnp.where(q < HALF, 2 * q, 2 * GS + 1 - 2 * q)
        place = jnp.where(q == HALF, 1, place) + GS * (at // packed)
        spread[half] = placed(nx * packed, z.ch, place, (q >= 0) & (q < GS))
    loads[0].wait()
    loads[1].wait()
    hb = z.blk // 2
    lo, hi = pl.ds(0, hb), pl.ds(hb, hb)
    side = lax.broadcasted_iota(jnp.int32, (GS, packed), 0)
    everywhere = side >= 0
    wpk[h, x, zz, yy] = (
        dot(wt_ref[:hb], placed(GS, packed, side, everywhere))
        + dot(wt_ref[hb:], placed(GS, packed, side + GS, everywhere))
    ).astype(BF16)
    xbuf[x] = wi_ref[...]
    pl.semaphore_wait(barrier, nx + ny + nz - 2)

    for d in range(1, nx):
        px = lax.rem(x + d, nx)
        send(wi_ref, xbuf.at[x], x_send, x_recv, r, 2 * px + h)
    send(tok_hbm, tok.at[h], swap_send, swap_recv, r, other)
    mine = wpk.at[h, x]

    @pl.when(h == 0)
    def _():
        for d in range(1, ny):
            py = lax.rem(yy + d, ny)
            send(mine.at[zz, yy], mine.at[zz, yy], wo_send.at[0], wo_recv.at[0], zz * ny + py, c)

    @pl.when(h == 1)
    def _():
        for d in range(1, nz):
            pz = lax.rem(zz + d, nz)
            send(mine.at[zz, yy], mine.at[zz, yy], wo_send.at[0], wo_recv.at[0], pz * ny + yy, c)

    chan_at = lax.broadcasted_iota(jnp.int32, (GS, z.ch), 0)
    drain(xbuf.at[pl.ds(0, nx - 1)], x_recv)
    total = dot(xbuf[0], placed(GS, z.ch, chan_at, chan_at >= 0))
    for n in range(1, nx):
        total += dot(xbuf[n], placed(GS, z.ch, chan_at + GS * n, chan_at >= 0))
    win[zz, yy] = total.astype(BF16)

    for d in range(1, ny):
        py = lax.rem(yy + d, ny)
        send(win.at[zz, yy, lo], win.at[zz, yy, lo], in_send.at[0], in_recv.at[0], zz * ny + py, c)
    for d in range(1, nz):
        pz = lax.rem(zz + d, nz)
        send(win.at[zz, yy, hi], win.at[zz, yy, hi], in_send.at[1], in_recv.at[1], pz * ny + yy, c)
    loads[2].wait()
    gain = gain_ref[...].astype(F32).reshape(1, z.width)
    step = min(32, local)

    def norm(q):
        def one(i, carry):
            part = pl.ds(pl.multiple_of(i * step, step), step)
            v = tok[q, part, :].astype(F32)
            inv = lax.rsqrt(jnp.mean(v * v, axis=-1, keepdims=True) + EPS)
            tok[q, part, :] = (v * inv * gain).astype(BF16)
            return carry

        lax.fori_loop(0, local // step, one, 0)

    own.wait()
    norm(h)

    @pl.when(h == 0)
    def _():
        drain(wpk.at[0, 0, 0, pl.ds(0, ny - 1)], wo_recv.at[0])
        for d in range(1, nz):
            pz = lax.rem(zz + d, nz)
            send(mine.at[zz], mine.at[zz], wo_send.at[1], wo_recv.at[1], pz * ny + yy, c)

    @pl.when(h == 1)
    def _():
        drain(wpk.at[0, 0, pl.ds(0, nz - 1), 0], wo_recv.at[0])
        for d in range(1, ny):
            py = lax.rem(yy + d, ny)
            send(mine.at[:, yy], mine.at[:, yy], wo_send.at[1], wo_recv.at[1], zz * ny + py, c)

    drain(win.at[0, pl.ds(0, ny - 1), lo], in_recv.at[0])
    drain(win.at[pl.ds(0, nz - 1), 0, hi], in_recv.at[1])
    cy, cz = min(z.cut, ny), min(z.cut, nz)

    def low(block, chunk):
        return win.at[block, pl.ds(chunk * (ny // cy), ny // cy), lo]

    def high(block, chunk):
        return win.at[pl.ds(chunk * (nz // cz), nz // cz), block, hi]

    def row_z(p):
        return p * ny + yy

    def row_y(p):
        return zz * ny + p

    paths = ((low, nz, zz, cy, row_z), (high, ny, yy, cz, row_y))

    def carried(n, cut, hop, sign):
        if hop < n // 2:
            return range(cut)
        return range(cut // 2) if sign > 0 else range(cut // 2, cut)

    longest = max(nz, ny) // 2
    line8 = nz == 8 and ny == 8

    def hand(view, chunk, block, p, e, kind, to, row):
        send(view(block, chunk), view(block, chunk), in_send.at[2 + p],
             ring_recv.at[p, e, kind, chunk], row(to), c)

    def start8():
        for chunk in range(z.cut):
            for far in (2, 1):
                for p, (view, n, pos, cut, row) in enumerate(paths):
                    for e, sign in enumerate((1, -1)):
                        hand(view, chunk, pos, p, e, far - 1, lax.rem(pos + far * sign + n, n), row)

    def relay8():
        for chunk in range(z.cut):
            for p, (view, n, pos, cut, row) in enumerate(paths):
                for e, sign in enumerate((1, -1)):
                    block = lax.rem(pos - 2 * sign + n, n)
                    drain(view(block, chunk), ring_recv.at[p, e, 1, chunk])
                    hand(view, chunk, block, p, e, 2, lax.rem(pos + sign + n, n), row)
                    if chunk in carried(n, cut, n // 2, sign):
                        hand(view, chunk, block, p, e, 3, lax.rem(pos + 2 * sign + n, n), row)

    def finish8():
        for kind in (0, 2, 3):
            for chunk in range(z.cut):
                for p, (view, n, pos, cut, row) in enumerate(paths):
                    for e, sign in enumerate((1, -1)):
                        if kind < 3 or chunk in carried(n, cut, n // 2, sign):
                            drain(view(pos, chunk), ring_recv.at[p, e, kind, chunk])

    def advance(hop):
        for chunk in range(max(cy, cz)):
            for p, (view, n, pos, cut, row) in enumerate(paths):
                for e, sign in enumerate((1, -1)):
                    block = lax.rem(pos - sign * (hop - 1) + n, n)
                    if 1 < hop <= n // 2 + 1 and chunk in carried(n, cut, hop - 1, sign):
                        drain(view(block, chunk), ring_recv.at[p, e, hop - 2, chunk])
                    if hop <= n // 2 and chunk in carried(n, cut, hop, sign):
                        to = lax.rem(pos + sign + n, n)
                        send(view(block, chunk), view(block, chunk), in_send.at[2 + p],
                             ring_recv.at[p, e, hop - 1, chunk], row(to), c)

    if line8:
        start8()
    else:
        advance(1)

    drain(tok.at[0], swap_recv)
    norm(1 - h)
    if line8:
        with jax.named_scope("pring2"):
            relay8()
        with jax.named_scope("pring3"):
            finish8()
    else:
        for hop in range(2, longest + 2):
            advance(hop)

    pl.semaphore_signal(plane_sem, inc=1, device_id=(r, other), device_id_type=MESH)

    @pl.when(h == 0)
    def _():
        drain(wpk.at[0, 0, pl.ds(0, nz - 1)], wo_recv.at[1])

    @pl.when(h == 1)
    def _():
        drain(wpk.at[0, 0, :, pl.ds(0, ny - 1)], wo_recv.at[1])

    near = (1, nx - 1) if nx == 4 else tuple(range(1, nx))
    for n, d in enumerate(near):
        px = lax.rem(x + d, nx)
        send(mine, mine, far_send, far_recv.at[n], r, 2 * px + h)
    send(mine, mine, half_send, half_recv.at[0], r, other)

    loads[3].wait()
    o1 = local
    o2 = o1 + 8 * rows
    o3 = o2 + z.ch
    chan = tab[o2:o3, :z.ch]
    weight = win[...].reshape(z.width, z.ch)
    for q in (1, 0):
        proj = dot(tok[q], weight).astype(BF16)
        cols = dot_nt(chan, proj).astype(BF16)
        ht[pl.ds(groups * q, groups)] = cols.reshape(groups, z.per, local)

        def scatter(i, carry):
            peer = groups * q + lax.rem(r + i, groups)

            @pl.when(peer != r)
            def _():
                send(ht.at[peer], got.at[r], a_send, a_recv, peer, c)

            return carry

        lax.fori_loop(0, groups, scatter, 0)
    got[r] = ht[r]

    zh = nz // 2
    for n, d in enumerate(near):
        theirs = wpk.at[h, lax.rem(x - d + nx, nx)]
        drain(theirs, far_recv.at[n])
        if nx == 4:
            part = pl.ds(n * zh, zh)
            to = lax.rem(x + d, nx)
            send(theirs.at[part], theirs.at[part], far_send, far_recv.at[2 + n], r, 2 * to + h)
        send(theirs, theirs, half_send, half_recv.at[1 + n], r, other)

    drain(got.at[pl.ds(0, rows - 1)], a_recv)

    if nx == 4:
        far = lax.rem(x + 2, nx)
        for n in range(2):
            part = wpk.at[h, far, pl.ds(n * zh, zh)]
            drain(part, far_recv.at[2 + n])
            send(part, part, half_send, half_recv.at[3], r, other)

    lane = z.lane
    for l in range(z.tiles):
        part = got[:, :, l * lane:(l + 1) * lane].astype(F32)
        stage[l] = part.reshape(rows * z.per, lane)
    base = lax.rem(r, groups) * z.pairs
    plain = tab[o1:o1 + 4 * rows, :2 * rows]
    for p in range(z.pairs):
        matrix = plain
        if p % min(z.pairs, HALF) == 0:
            paired = tab[o1 + 4 * rows:o2, :2 * rows].astype(F32)
            special = lax.rem(base + p, HALF) == 0
            matrix = jnp.where(special, paired, plain.astype(F32)).astype(BF16)
        for l in range(z.tiles):
            lanes = slice(l * lane, (l + 1) * lane)
            rest = slice(local + l * lane, local + (l + 1) * lane)
            cos = tab[o3:o3 + rows, lanes].astype(F32) + tab[o3:o3 + rows, rest].astype(F32)
            sin = (tab[o3 + rows:o3 + 2 * rows, lanes].astype(F32)
                   + tab[o3 + rows:o3 + 2 * rows, rest].astype(F32))
            u = stage[l, pl.ds(2 * p, rows, stride=z.per), :]
            v = stage[l, pl.ds(2 * p + 1, rows, stride=z.per), :]
            g = dot(matrix, jnp.concatenate([u, v], axis=0).astype(BF16))
            for w in range(2):
                re = g[2 * w * rows:(2 * w + 1) * rows]
                im = g[(2 * w + 1) * rows:(2 * w + 2) * rows]
                at = pl.ds((2 * p + w) * rows, rows)
                gp[at, lanes] = (re * cos + im * sin).astype(BF16)
                gp[at, rest] = (im * cos - re * sin).astype(BF16)
    spec = dot_nt(tab[:local], gp[...])
    if rows == GS and lane == 128:
        left = lax.broadcasted_iota(jnp.int32, (rows, lane), 1) < rows
        for l in range(z.tiles):
            for p in range(z.pairs):
                t0 = spec[2 * l * rows:(2 * l + 1) * rows, p * lane:(p + 1) * lane]
                t1 = spec[(2 * l + 1) * rows:(2 * l + 2) * rows, p * lane:(p + 1) * lane]
                stage[l, pl.ds(2 * p, rows, stride=z.per), :] = jnp.where(
                    left, t0, pltpu.roll(t1, rows, 1)
                )
                stage[l, pl.ds(2 * p + 1, rows, stride=z.per), :] = jnp.where(
                    left, pltpu.roll(t0, rows, 1), t1
                )
    else:
        full = spec.reshape(z.hops, rows, z.per, rows).transpose(1, 2, 0, 3)
        full = full.reshape(rows * z.per, z.tiles, lane)
        for l in range(z.tiles):
            stage[l] = full[:, l]
    for l in range(z.tiles):
        back[:, :, l * lane:(l + 1) * lane] = stage[l].reshape(rows, z.per, lane).astype(BF16)

    pl.semaphore_wait(plane_sem, 1)
    seq = r // groups
    slot = h * groups + lax.rem(r, groups)
    target = 2 * x + seq

    for k in range(nz):
        pz = k // 2 + (k % 2) * (nz // 2)

        def give(i, carry, pz=pz):
            peer = pz * ny + lax.rem(yy + i, ny)
            send(back.at[peer], got2.at[slot], b_send, b_recv, peer, target)
            return carry

        lax.fori_loop(1, ny, give, 0)

        @pl.when(pz != zz)
        def _(pz=pz, give=give):
            give(0, 0)

    @pl.when(seq == h)
    def _():
        got2[slot] = back[r]

    @pl.when(seq != h)
    def _():
        send(back.at[r], got2.at[slot], b_send, b_recv, r, target)

    def unpack(half_of):
        flat = jnp.concatenate(
            [wpk[half_of, n].reshape(rows * hb, packed) for n in range(nx)], axis=1
        )
        for half in range(2):
            sorted_ = dot(flat, spread[half]).astype(BF16)
            wo[half_of, :, half * hb:(half + 1) * hb, :] = sorted_.reshape(rows, hb, z.ch)

    unpack(h)
    for n in range(nx):
        drain(wpk.at[0, 0], half_recv.at[n])
    unpack(1 - h)

    @pl.when(seq == h)
    def _():
        drain(got2.at[pl.ds(0, rows - 1)], b_recv)

    @pl.when(seq != h)
    def _():
        drain(got2, b_recv)

    mixed = got2[...].astype(F32).reshape(rows * z.per, local).T.astype(BF16)
    ma, mb = mixed[:, :z.ch], mixed[:, z.ch:]
    chunk = ny * z.blk
    for n in range(nz):
        some = pl.ds(n * ny, ny)
        res = dot_nt(ma, wo[0, some].reshape(chunk, z.ch)) + dot_nt(mb, wo[1, some].reshape(chunk, z.ch))
        out[:, n * chunk:(n + 1) * chunk] = res.astype(BF16)

    drain(xbuf.at[pl.ds(0, nx - 1)], x_send)
    drain(tok.at[0], swap_send)
    drain(win.at[0, pl.ds(0, ny - 1), lo], in_send.at[0])
    drain(win.at[pl.ds(0, nz - 1), 0, hi], in_send.at[1])
    drain(win.at[pl.ds(0, nz - 1), :, lo], in_send.at[2])
    drain(win.at[:, pl.ds(0, ny - 1), hi], in_send.at[3])

    @pl.when(h == 0)
    def _():
        drain(wpk.at[0, 0, 0, pl.ds(0, ny - 1)], wo_send.at[0])
        drain(wpk.at[0, 0, pl.ds(0, nz - 1)], wo_send.at[1])

    @pl.when(h == 1)
    def _():
        drain(wpk.at[0, 0, pl.ds(0, nz - 1), 0], wo_send.at[0])
        drain(wpk.at[0, 0, :, pl.ds(0, ny - 1)], wo_send.at[1])

    drain(wpk.at[0, pl.ds(0, nx - 1)], far_send)
    drain(wpk.at[0], half_send)
    drain(ht.at[pl.ds(0, rows - 1)], a_send)

    @pl.when(seq == h)
    def _():
        drain(back.at[pl.ds(0, rows - 1)], b_send)

    @pl.when(seq != h)
    def _():
        drain(back, b_send)


def body(rows, cols, tokens, norm_gain, in_weight, out_weight):
    local, width = tokens.shape[1:]
    z = Sizes(rows, cols, local, width)
    table = tables(z)
    hbm = pl.BlockSpec(memory_space=pltpu.HBM)
    vmem = pl.BlockSpec(memory_space=pltpu.VMEM)
    hb = z.blk // 2
    dma = pltpu.SemaphoreType.DMA
    vm = pltpu.VMEM
    exchange = (rows, z.per, local)
    scratch = [
        vm((width,), BF16),
        vm((z.blk, GS), BF16),
        vm((z.blk, GS), BF16),
        vm(table.shape, BF16),
        vm((2, local, width), BF16),
        vm((z.nx, z.blk, GS), BF16),
        vm((z.nz, z.ny, z.blk, z.ch), BF16),
        vm((2, z.nx, z.nz, z.ny, hb, 2 * GS), BF16),
        vm((2, rows, z.blk, z.ch), BF16),
        vm((2, 2 * GS * z.nx, z.ch), BF16),
        vm(exchange, BF16),
        vm(exchange, BF16),
        vm((z.tiles, rows * z.per, z.lane), F32),
        vm((z.per * rows, 2 * local), BF16),
        vm(exchange, BF16),
        vm(exchange, BF16),
        dma((4,)), dma, dma, dma,
        dma, dma, dma((4,)), dma((2,)), dma((2, 2, max(z.ny, z.nz) // 2, z.cut)), dma((2,)), dma((2,)),
        dma, dma((4,)), dma, dma((4,)),
        dma, dma, dma, dma, pltpu.SemaphoreType.REGULAR,
    ]
    operands = (tokens[0], norm_gain, in_weight, out_weight.T, table)
    mixed = pl.pallas_call(
        functools.partial(kernel, z),
        out_shape=jax.ShapeDtypeStruct((local, width), BF16),
        in_specs=[hbm] * 5,
        out_specs=vmem,
        scratch_shapes=scratch,
        compiler_params=pltpu.CompilerParams(
            collective_id=0, has_side_effects=True, vmem_limit_bytes=VMEM_LIMIT
        ),
        name="fourier_mix",
    )(*(pltpu.with_memory_space_constraint(a, pltpu.HBM) for a in operands))
    return mixed[None]


def solution(mesh):
    rows, cols = mesh.shape["row"], mesh.shape["col"]
    in_specs = (P("col", "row", None), P(), P("row", "col"), P("col", "row"))
    return jax.shard_map(
        functools.partial(body, rows, cols), mesh=mesh, in_specs=in_specs,
        out_specs=P("col", "row", None), check_vma=False,
    )
```

```python
import functools
import math

import jax
import jax.numpy as jnp
import numpy as np
from jax import lax
from jax.experimental import pallas as pl
from jax.experimental.pallas import tpu as pltpu
from jax.sharding import PartitionSpec as P

GS = 64
HALF = GS // 2
EPS = 1e-06
F32 = jnp.float32
BF16 = jnp.bfloat16
MESH = pl.DeviceIdType.MESH
VMEM_LIMIT = 52 * 1024 * 1024


class Sizes:
    def __init__(self, rows, cols, local, width):
        self.rows = rows
        self.nz = 1 << ((rows.bit_length() - 1 + 1) // 2)
        self.ny = rows // self.nz
        self.nx = cols // 2
        self.local = local
        self.width = width
        self.ch = GS * self.nx
        self.per = 2 * self.ch // rows
        self.pairs = self.per // 2
        self.hops = local // rows
        self.blk = width // rows
        self.cut = 4
        self.tiles = max(1, local // 128)
        self.lane = local // self.tiles


def tables(z):
    rows, local, ch = z.rows, z.local, z.ch
    length = rows * local
    k = np.arange(GS)
    small = np.zeros((GS, GS))
    for j in range(HALF):
        if j == 0:
            small[0] = (1.0 + (-1.0) ** k) / 2
            small[1] = (1.0 - (-1.0) ** k) / 2
        else:
            small[2 * j] = np.cos(2 * math.pi * j * k / GS)
            small[2 * j + 1] = np.sin(2 * math.pi * j * k / GS)
    chan = np.kron(np.eye(z.nx), small)
    i = np.arange(rows)
    ang = 2 * math.pi * (np.outer(i, i) % rows) / rows
    c, s = np.cos(ang), np.sin(ang)
    first = np.concatenate(
        [
            np.block([[c, -s], [-s, -c], [c, s], [-s, c]]),
            np.block([[c, c], [-s, -s], [c, -c], [-s, s]]),
        ]
    )
    m = np.arange(local)
    tw = 2 * math.pi * np.outer(i, m) / length
    turn = np.concatenate([np.cos(tw), np.sin(tw)]).astype(np.float32)
    high = turn.astype(BF16).astype(np.float32)
    turn = np.concatenate([high, turn - high], axis=1)
    a = np.arange(z.hops)
    k2 = z.hops * i.reshape(2, 1, rows // 2) + a[None, :, None]
    k2 = k2.reshape(-1)
    ang2 = 2 * math.pi * (np.outer(k2, m) % local) / local
    second = np.concatenate([np.cos(ang2), np.sin(ang2)], axis=1) / math.sqrt(length * GS)
    parts = []
    for part in (second, first, chan, turn):
        wide = np.zeros((part.shape[0], 2 * local), np.float32)
        wide[:, : part.shape[1]] = part
        parts.append(wide)
    return jnp.asarray(np.concatenate(parts).astype(BF16))


def dot(a, b):
    return jnp.dot(a, b, preferred_element_type=F32)


def dot_nt(a, b):
    return lax.dot_general(a, b, (((1,), (1,)), ((), ())), preferred_element_type=F32)


def placed(rows, cols, target, keep):
    to = lax.broadcasted_iota(jnp.int32, (rows, cols), 1)
    return jnp.where((to == target) & keep, 1.0, 0.0).astype(BF16)


def kernel(
    z,
    tok_hbm, gain_hbm, wi_hbm, wt_hbm, tab_hbm,
    out,
    gain_ref, wi_ref, wt_ref, tab, tok,
    xbuf, win, wpk, wo, spread, ht, got, stage, gp, back, got2,
    tab_sem, tok_sem, swap_send, swap_recv,
    x_send, x_recv, in_send, in_recv, ring_recv, wo_send, wo_recv,
    far_send, far_recv, half_send, half_recv,
    a_send, a_recv, b_send, b_recv, plane_sem,
):
    rows, ny, nz, nx, local = z.rows, z.ny, z.nz, z.nx, z.local
    groups = rows // 2
    r = lax.axis_index("row")
    c = lax.axis_index("col")
    h = lax.rem(c, 2)
    x = c // 2
    zz = r // ny
    yy = lax.rem(r, ny)
    other = c + 1 - 2 * h

    def send(src, dst, ssem, rsem, row, col):
        copy = pltpu.make_async_remote_copy(
            src_ref=src, dst_ref=dst, send_sem=ssem, recv_sem=rsem,
            device_id=(row, col), device_id_type=MESH,
        )
        copy.start()

    def drain(ref, sem):
        pltpu.make_async_copy(ref, ref, sem).wait()

    barrier = pltpu.get_barrier_semaphore()
    loads = [
        pltpu.make_async_copy(src, dst, tab_sem.at[n])
        for n, (src, dst) in enumerate(
            [(wi_hbm, wi_ref), (wt_hbm, wt_ref), (gain_hbm, gain_ref), (tab_hbm, tab)]
        )
    ]
    for load in loads[:2]:
        load.start()

    for d in range(1, nx):
        px = lax.rem(x + d, nx)
        pl.semaphore_signal(barrier, inc=1, device_id=(r, 2 * px + h), device_id_type=MESH)
    for d in range(1, ny):
        to = zz * ny + lax.rem(yy + d, ny)
        pl.semaphore_signal(barrier, inc=1, device_id=(to, c), device_id_type=MESH)
    for d in range(1, nz):
        to = lax.rem(zz + d, nz) * ny + yy
        pl.semaphore_signal(barrier, inc=1, device_id=(to, c), device_id_type=MESH)
    pl.semaphore_signal(barrier, inc=1, device_id=(r, other), device_id_type=MESH)

    own = pltpu.make_async_copy(tok_hbm, tok.at[h], tok_sem)
    own.start()
    for load in loads[2:]:
        load.start()
    packed = 2 * GS
    at = lax.broadcasted_iota(jnp.int32, (nx * packed, z.ch), 0)
    for half in range(2):
        q = lax.rem(at, packed) - GS * half
        place = jnp.where(q < HALF, 2 * q, 2 * GS + 1 - 2 * q)
        place = jnp.where(q == HALF, 1, place) + GS * (at // packed)
        spread[half] = placed(nx * packed, z.ch, place, (q >= 0) & (q < GS))
    loads[0].wait()
    loads[1].wait()
    hb = z.blk // 2
    lo, hi = pl.ds(0, hb), pl.ds(hb, hb)
    side = lax.broadcasted_iota(jnp.int32, (GS, packed), 0)
    everywhere = side >= 0
    wpk[h, x, zz, yy] = (
        dot(wt_ref[:hb], placed(GS, packed, side, everywhere))
        + dot(wt_ref[hb:], placed(GS, packed, side + GS, everywhere))
    ).astype(BF16)
    xbuf[x] = wi_ref[...]
    pl.semaphore_wait(barrier, nx + ny + nz - 2)

    for d in range(1, nx):
        px = lax.rem(x + d, nx)
        send(wi_ref, xbuf.at[x], x_send, x_recv, r, 2 * px + h)
    send(tok_hbm, tok.at[h], swap_send, swap_recv, r, other)
    mine = wpk.at[h, x]

    @pl.when(h == 0)
    def _():
        for d in range(1, ny):
            py = lax.rem(yy + d, ny)
            send(mine.at[zz, yy], mine.at[zz, yy], wo_send.at[0], wo_recv.at[0], zz * ny + py, c)

    @pl.when(h == 1)
    def _():
        for d in range(1, nz):
            pz = lax.rem(zz + d, nz)
            send(mine.at[zz, yy], mine.at[zz, yy], wo_send.at[0], wo_recv.at[0], pz * ny + yy, c)

    chan_at = lax.broadcasted_iota(jnp.int32, (GS, z.ch), 0)
    drain(xbuf.at[pl.ds(0, nx - 1)], x_recv)
    total = dot(xbuf[0], placed(GS, z.ch, chan_at, chan_at >= 0))
    for n in range(1, nx):
        total += dot(xbuf[n], placed(GS, z.ch, chan_at + GS * n, chan_at >= 0))
    win[zz, yy] = total.astype(BF16)

    for d in range(1, ny):
        py = lax.rem(yy + d, ny)
        send(win.at[zz, yy, lo], win.at[zz, yy, lo], in_send.at[0], in_recv.at[0], zz * ny + py, c)
    for d in range(1, nz):
        pz = lax.rem(zz + d, nz)
        send(win.at[zz, yy, hi], win.at[zz, yy, hi], in_send.at[1], in_recv.at[1], pz * ny + yy, c)
    loads[2].wait()
    gain = gain_ref[...].astype(F32).reshape(1, z.width)
    step = min(32, local)

    def norm(q):
        def one(i, carry):
            part = pl.ds(pl.multiple_of(i * step, step), step)
            v = tok[q, part, :].astype(F32)
            inv = lax.rsqrt(jnp.mean(v * v, axis=-1, keepdims=True) + EPS)
            tok[q, part, :] = (v * inv * gain).astype(BF16)
            return carry

        lax.fori_loop(0, local // step, one, 0)

    own.wait()
    norm(h)

    @pl.when(h == 0)
    def _():
        drain(wpk.at[0, 0, 0, pl.ds(0, ny - 1)], wo_recv.at[0])
        for d in range(1, nz):
            pz = lax.rem(zz + d, nz)
            send(mine.at[zz], mine.at[zz], wo_send.at[1], wo_recv.at[1], pz * ny + yy, c)

    @pl.when(h == 1)
    def _():
        drain(wpk.at[0, 0, pl.ds(0, nz - 1), 0], wo_recv.at[0])
        for d in range(1, ny):
            py = lax.rem(yy + d, ny)
            send(mine.at[:, yy], mine.at[:, yy], wo_send.at[1], wo_recv.at[1], zz * ny + py, c)

    drain(win.at[0, pl.ds(0, ny - 1), lo], in_recv.at[0])
    drain(win.at[pl.ds(0, nz - 1), 0, hi], in_recv.at[1])
    cy, cz = min(z.cut, ny), min(z.cut, nz)

    def low(block, chunk):
        return win.at[block, pl.ds(chunk * (ny // cy), ny // cy), lo]

    def high(block, chunk):
        return win.at[pl.ds(chunk * (nz // cz), nz // cz), block, hi]

    def row_z(p):
        return p * ny + yy

    def row_y(p):
        return zz * ny + p

    paths = ((low, nz, zz, cy, row_z), (high, ny, yy, cz, row_y))

    def carried(n, cut, hop, sign):
        if hop < n // 2:
            return range(cut)
        return range(cut // 2) if sign > 0 else range(cut // 2, cut)

    longest = max(nz, ny) // 2
    line8 = nz == 8 and ny == 8

    def hand(view, chunk, block, p, e, kind, to, row):
        send(view(block, chunk), view(block, chunk), in_send.at[2 + p],
             ring_recv.at[p, e, kind, chunk], row(to), c)

    def start8():
        for chunk in range(z.cut):
            for far in (2, 1):
                for p, (view, n, pos, cut, row) in enumerate(paths):
                    for e, sign in enumerate((1, -1)):
                        hand(view, chunk, pos, p, e, far - 1, lax.rem(pos + far * sign + n, n), row)

    def relay8():
        for chunk in range(z.cut):
            for p, (view, n, pos, cut, row) in enumerate(paths):
                for e, sign in enumerate((1, -1)):
                    block = lax.rem(pos - 2 * sign + n, n)
                    drain(view(block, chunk), ring_recv.at[p, e, 1, chunk])
                    hand(view, chunk, block, p, e, 2, lax.rem(pos + sign + n, n), row)
                    if chunk in carried(n, cut, n // 2, sign):
                        hand(view, chunk, block, p, e, 3, lax.rem(pos + 2 * sign + n, n), row)

    def finish8():
        for kind in (0, 2, 3):
            for chunk in range(z.cut):
                for p, (view, n, pos, cut, row) in enumerate(paths):
                    for e, sign in enumerate((1, -1)):
                        if kind < 3 or chunk in carried(n, cut, n // 2, sign):
                            drain(view(pos, chunk), ring_recv.at[p, e, kind, chunk])

    def advance(hop):
        for chunk in range(max(cy, cz)):
            for p, (view, n, pos, cut, row) in enumerate(paths):
                for e, sign in enumerate((1, -1)):
                    block = lax.rem(pos - sign * (hop - 1) + n, n)
                    if 1 < hop <= n // 2 + 1 and chunk in carried(n, cut, hop - 1, sign):
                        drain(view(block, chunk), ring_recv.at[p, e, hop - 2, chunk])
                    if hop <= n // 2 and chunk in carried(n, cut, hop, sign):
                        to = lax.rem(pos + sign + n, n)
                        send(view(block, chunk), view(block, chunk), in_send.at[2 + p],
                             ring_recv.at[p, e, hop - 1, chunk], row(to), c)

    if line8:
        start8()
    else:
        advance(1)

    drain(tok.at[0], swap_recv)
    norm(1 - h)
    if line8:
        with jax.named_scope("pring2"):
            relay8()
        with jax.named_scope("pring3"):
            finish8()
    else:
        for hop in range(2, longest + 2):
            advance(hop)

    pl.semaphore_signal(plane_sem, inc=1, device_id=(r, other), device_id_type=MESH)

    @pl.when(h == 0)
    def _():
        drain(wpk.at[0, 0, pl.ds(0, nz - 1)], wo_recv.at[1])

    @pl.when(h == 1)
    def _():
        drain(wpk.at[0, 0, :, pl.ds(0, ny - 1)], wo_recv.at[1])

    near = (1, nx - 1) if nx == 4 else tuple(range(1, nx))
    for n, d in enumerate(near):
        px = lax.rem(x + d, nx)
        send(mine, mine, far_send, far_recv.at[n], r, 2 * px + h)
    send(mine, mine, half_send, half_recv.at[0], r, other)

    loads[3].wait()
    o1 = local
    o2 = o1 + 8 * rows
    o3 = o2 + z.ch
    chan = tab[o2:o3, :z.ch]
    weight = win[...].reshape(z.width, z.ch)
    for q in (1, 0):
        proj = dot(tok[q], weight).astype(BF16)
        cols = dot_nt(chan, proj).astype(BF16)
        ht[pl.ds(groups * q, groups)] = cols.reshape(groups, z.per, local)

        def scatter(i, carry):
            peer = groups * q + lax.rem(r + i, groups)

            @pl.when(peer != r)
            def _():
                send(ht.at[peer], got.at[r], a_send, a_recv, peer, c)

            return carry

        lax.fori_loop(0, groups, scatter, 0)
    got[r] = ht[r]

    zh = nz // 2
    for n, d in enumerate(near):
        theirs = wpk.at[h, lax.rem(x - d + nx, nx)]
        drain(theirs, far_recv.at[n])
        if nx == 4:
            part = pl.ds(n * zh, zh)
            to = lax.rem(x + d, nx)
            send(theirs.at[part], theirs.at[part], far_send, far_recv.at[2 + n], r, 2 * to + h)
        send(theirs, theirs, half_send, half_recv.at[1 + n], r, other)

    drain(got.at[pl.ds(0, rows - 1)], a_recv)

    if nx == 4:
        far = lax.rem(x + 2, nx)
        for n in range(2):
            part = wpk.at[h, far, pl.ds(n * zh, zh)]
            drain(part, far_recv.at[2 + n])
            send(part, part, half_send, half_recv.at[3], r, other)

    lane = z.lane
    for l in range(z.tiles):
        part = got[:, :, l * lane:(l + 1) * lane].astype(F32)
        stage[l] = part.reshape(rows * z.per, lane)
    base = lax.rem(r, groups) * z.pairs
    plain = tab[o1:o1 + 4 * rows, :2 * rows]
    for p in range(z.pairs):
        matrix = plain
        if p % min(z.pairs, HALF) == 0:
            paired = tab[o1 + 4 * rows:o2, :2 * rows].astype(F32)
            special = lax.rem(base + p, HALF) == 0
            matrix = jnp.where(special, paired, plain.astype(F32)).astype(BF16)
        for l in range(z.tiles):
            lanes = slice(l * lane, (l + 1) * lane)
            rest = slice(local + l * lane, local + (l + 1) * lane)
            cos = tab[o3:o3 + rows, lanes].astype(F32) + tab[o3:o3 + rows, rest].astype(F32)
            sin = (tab[o3 + rows:o3 + 2 * rows, lanes].astype(F32)
                   + tab[o3 + rows:o3 + 2 * rows, rest].astype(F32))
            u = stage[l, pl.ds(2 * p, rows, stride=z.per), :]
            v = stage[l, pl.ds(2 * p + 1, rows, stride=z.per), :]
            g = dot(matrix, jnp.concatenate([u, v], axis=0).astype(BF16))
            for w in range(2):
                re = g[2 * w * rows:(2 * w + 1) * rows]
                im = g[(2 * w + 1) * rows:(2 * w + 2) * rows]
                at = pl.ds((2 * p + w) * rows, rows)
                gp[at, lanes] = (re * cos + im * sin).astype(BF16)
                gp[at, rest] = (im * cos - re * sin).astype(BF16)
    pl.semaphore_wait(plane_sem, 1)
    seq = r // groups
    slot = h * groups + lax.rem(r, groups)
    target = 2 * x + seq
    hr = rows // 2
    for half in range(2):
        spec = dot_nt(tab[half * (local // 2):(half + 1) * (local // 2)], gp[...])
        if rows == GS and lane == 128:
            left = lax.broadcasted_iota(jnp.int32, (hr, lane), 1) < rows
            for l in range(z.tiles):
                for p in range(z.pairs):
                    t0 = spec[2 * l * hr:(2 * l + 1) * hr, p * lane:(p + 1) * lane]
                    t1 = spec[(2 * l + 1) * hr:(2 * l + 2) * hr, p * lane:(p + 1) * lane]
                    at = half * hr * z.per + 2 * p
                    stage[l, pl.ds(at, hr, stride=z.per), :] = jnp.where(
                        left, t0, pltpu.roll(t1, rows, 1)
                    )
                    stage[l, pl.ds(at + 1, hr, stride=z.per), :] = jnp.where(
                        left, pltpu.roll(t0, rows, 1), t1
                    )
        else:
            full = spec.reshape(z.hops, hr, z.per, rows).transpose(1, 2, 0, 3)
            full = full.reshape(hr * z.per, z.tiles, lane)
            for l in range(z.tiles):
                stage[l, half * hr * z.per:(half + 1) * hr * z.per] = full[:, l]
        for l in range(z.tiles):
            part = stage[l, half * hr * z.per:(half + 1) * hr * z.per]
            back[half * hr:(half + 1) * hr, :, l * lane:(l + 1) * lane] = part.reshape(
                hr, z.per, lane
            ).astype(BF16)
        for pz in range(half * (nz // 2), (half + 1) * (nz // 2)):

            def give(i, carry, pz=pz):
                peer = pz * ny + lax.rem(yy + i, ny)
                send(back.at[peer], got2.at[slot], b_send, b_recv, peer, target)
                return carry

            lax.fori_loop(1, ny, give, 0)

            @pl.when(pz != zz)
            def _(give=give):
                give(0, 0)

    @pl.when(seq == h)
    def _():
        got2[slot] = back[r]

    @pl.when(seq != h)
    def _():
        send(back.at[r], got2.at[slot], b_send, b_recv, r, target)

    def unpack(half_of):
        flat = jnp.concatenate(
            [wpk[half_of, n].reshape(rows * hb, packed) for n in range(nx)], axis=1
        )
        for half in range(2):
            sorted_ = dot(flat, spread[half]).astype(BF16)
            wo[half_of, :, half * hb:(half + 1) * hb, :] = sorted_.reshape(rows, hb, z.ch)

    unpack(h)
    for n in range(nx):
        drain(wpk.at[0, 0], half_recv.at[n])
    unpack(1 - h)

    @pl.when(seq == h)
    def _():
        drain(got2.at[pl.ds(0, rows - 1)], b_recv)

    @pl.when(seq != h)
    def _():
        drain(got2, b_recv)

    mixed = got2[...].astype(F32).reshape(rows * z.per, local).T.astype(BF16)
    ma, mb = mixed[:, :z.ch], mixed[:, z.ch:]
    chunk = ny * z.blk
    for n in range(nz):
        some = pl.ds(n * ny, ny)
        res = dot_nt(ma, wo[0, some].reshape(chunk, z.ch)) + dot_nt(mb, wo[1, some].reshape(chunk, z.ch))
        out[:, n * chunk:(n + 1) * chunk] = res.astype(BF16)

    drain(xbuf.at[pl.ds(0, nx - 1)], x_send)
    drain(tok.at[0], swap_send)
    drain(win.at[0, pl.ds(0, ny - 1), lo], in_send.at[0])
    drain(win.at[pl.ds(0, nz - 1), 0, hi], in_send.at[1])
    drain(win.at[pl.ds(0, nz - 1), :, lo], in_send.at[2])
    drain(win.at[:, pl.ds(0, ny - 1), hi], in_send.at[3])

    @pl.when(h == 0)
    def _():
        drain(wpk.at[0, 0, 0, pl.ds(0, ny - 1)], wo_send.at[0])
        drain(wpk.at[0, 0, pl.ds(0, nz - 1)], wo_send.at[1])

    @pl.when(h == 1)
    def _():
        drain(wpk.at[0, 0, pl.ds(0, nz - 1), 0], wo_send.at[0])
        drain(wpk.at[0, 0, :, pl.ds(0, ny - 1)], wo_send.at[1])

    drain(wpk.at[0, pl.ds(0, nx - 1)], far_send)
    drain(wpk.at[0], half_send)
    drain(ht.at[pl.ds(0, rows - 1)], a_send)

    @pl.when(seq == h)
    def _():
        drain(back.at[pl.ds(0, rows - 1)], b_send)

    @pl.when(seq != h)
    def _():
        drain(back, b_send)


def body(rows, cols, tokens, norm_gain, in_weight, out_weight):
    local, width = tokens.shape[1:]
    z = Sizes(rows, cols, local, width)
    table = tables(z)
    hbm = pl.BlockSpec(memory_space=pltpu.HBM)
    vmem = pl.BlockSpec(memory_space=pltpu.VMEM)
    hb = z.blk // 2
    dma = pltpu.SemaphoreType.DMA
    vm = pltpu.VMEM
    exchange = (rows, z.per, local)
    scratch = [
        vm((width,), BF16),
        vm((z.blk, GS), BF16),
        vm((z.blk, GS), BF16),
        vm(table.shape, BF16),
        vm((2, local, width), BF16),
        vm((z.nx, z.blk, GS), BF16),
        vm((z.nz, z.ny, z.blk, z.ch), BF16),
        vm((2, z.nx, z.nz, z.ny, hb, 2 * GS), BF16),
        vm((2, rows, z.blk, z.ch), BF16),
        vm((2, 2 * GS * z.nx, z.ch), BF16),
        vm(exchange, BF16),
        vm(exchange, BF16),
        vm((z.tiles, rows * z.per, z.lane), F32),
        vm((z.per * rows, 2 * local), BF16),
        vm(exchange, BF16),
        vm(exchange, BF16),
        dma((4,)), dma, dma, dma,
        dma, dma, dma((4,)), dma((2,)), dma((2, 2, max(z.ny, z.nz) // 2, z.cut)), dma((2,)), dma((2,)),
        dma, dma((4,)), dma, dma((4,)),
        dma, dma, dma, dma, pltpu.SemaphoreType.REGULAR,
    ]
    operands = (tokens[0], norm_gain, in_weight, out_weight.T, table)
    mixed = pl.pallas_call(
        functools.partial(kernel, z),
        out_shape=jax.ShapeDtypeStruct((local, width), BF16),
        in_specs=[hbm] * 5,
        out_specs=vmem,
        scratch_shapes=scratch,
        compiler_params=pltpu.CompilerParams(
            collective_id=0, has_side_effects=True, vmem_limit_bytes=VMEM_LIMIT
        ),
        name="fourier_mix",
    )(*(pltpu.with_memory_space_constraint(a, pltpu.HBM) for a in operands))
    return mixed[None]


def solution(mesh):
    rows, cols = mesh.shape["row"], mesh.shape["col"]
    in_specs = (P("col", "row", None), P(), P("row", "col"), P("col", "row"))
    return jax.shard_map(
        functools.partial(body, rows, cols), mesh=mesh, in_specs=in_specs,
        out_specs=P("col", "row", None), check_vma=False,
    )
```
